256 devices in a mesh: grp: 2 (over y), fs: 16 (over z), tp: 8 (over x, core).
Axes of the slice: x: 4, y: 2, z: 16, core: 2. Of those that a mesh axis runs over, the one named last changes fastest.
The devices are a block of a 4x16x16 slice.
Arguments:
- tokens: bfloat16 [32768, 2048], P(('grp', 'fs'), 'tp'), parts along dimension 0, may hold values from -50 to 50
- mix_gain: float32 [2048], replicated, may hold values from 0.1 to 1.9
- value_proj: bfloat16 [2048, 1024], P('fs', 'tp'), may hold values from -0.125 to 0.125
- gate_proj: bfloat16 [2048, 1024], P('fs', 'tp'), may hold values from -0.125 to 0.125
- conv_taps: float32 [31, 1024], P(None, 'tp'), may hold values from -1 to 1
- chan_gain: float32 [1024], replicated, may hold values from 0.1 to 1.9
- chan_shift: float32 [1024], replicated, may hold values from -3 to 3
- mix_out: bfloat16 [1024, 2048], P('fs', 'tp'), may hold values from -0.1875 to 0.1875
- mlp_gain: float32 [2048], replicated, may hold values from 0.1 to 1.9
- mlp_gate: bfloat16 [2048, 5632], P('fs', 'tp'), may hold values from -0.125 to 0.125
- mlp_up: bfloat16 [2048, 5632], P('fs', 'tp'), may hold values from -0.125 to 0.125
- gate_taps: float32 [3, 5632], P(None, 'tp'), may hold values from -3.5 to 3.5
- up_taps: float32 [3, 5632], P(None, 'tp'), may hold values from -3.5 to 3.5
- mlp_down: bfloat16 [5632, 2048], P('tp', 'fs'), may hold values from -0.078125 to 0.078125
- final_gain: float32 [2048], P('tp'), may hold values from 0.1 to 1.9
Outputs:
- layer_out: bfloat16 [32768, 2048], P(('grp', 'fs'), 'tp'), parts along dimension 0
The draws below stay inside these ranges and needn't reach their ends.
There are 2 independent parts, one for each index of `grp`. The reference program is written for one: setup_inputs(seed, part) draws one part's arguments, and reference() takes and returns one part's arrays. A program takes and returns all parts, laid end to end along the dimension named above; an argument that names none is the same for every part. Nothing has to cross between parts.
All inputs are finite; a program needn't handle non-finite values.
Results may differ from the reference program's by a relative error of at most 0.0095.
Values may be sent and summed in bfloat16 or wider, within the bound.
No kernel may reach another device: no remote copies, remote signals or barrier semaphores. Data moves between devices by JAX's collectives and lax.ppermute only.
A program may use at most 128 MiB of HBM per device.

```python
import math
import jax
import jax.numpy as jnp
from jax import lax

D = 2048
CA = 1024
FF = 5632
KW = 31
FKW = 3
TOK_DEV = 1024
TOKENS = 16384
FF_BLOCK = 704
N_TP = 8


def draw_tokens(key, part):
    base_key = jax.random.fold_in(key, 7)
    key_rows, key_cols, key_vals = jax.random.split(base_key, 3)
    lowest = 0.3
    values = jnp.clip(jax.random.normal(key_vals, (TOKENS, D), jnp.float32), -4.0, 4.0)
    row_scale = jnp.exp(jax.random.uniform(key_rows, (TOKENS, 1), jnp.float32, math.log(lowest), math.log(3.0)))
    ramp = jnp.exp(jnp.linspace(math.log(0.4), math.log(2.5), D, dtype=jnp.float32))[None, :]
    col_scale = ramp * jnp.exp(jax.random.uniform(key_cols, (1, D), jnp.float32, -0.5, 0.5))
    return (values * row_scale * col_scale).astype(jnp.bfloat16)


def steps_of(key, dims, pieces, least, largest):
    level = 1.0
    for dim, blocks in pieces:
        draws = jax.random.uniform(jax.random.fold_in(jax.random.fold_in(key, 6), dim), (blocks,), jnp.float32, least / len(pieces), largest / len(pieces))
        level = level * jnp.repeat(jnp.exp(draws), dims[dim] // blocks).reshape((-1,) + (1,) * (len(dims) - 1 - dim))
    return level


def normal_values(own_key, extent, scale, reach, cuts=(), kind=jnp.bfloat16):
    array = scale * jax.random.normal(own_key, extent, jnp.float32)
    if cuts:
        array = array * steps_of(own_key, extent, cuts, -0.22, 0.18)
    return jnp.clip(array, -reach, reach).astype(kind)


def setup_inputs(seed: int = 0, part: int = 0) -> dict:
    splits = jax.random.split(jax.random.key(seed), 16)
    part_keys = jax.random.split(jax.random.fold_in(splits[15], part), 16)
    return {
        "tokens": draw_tokens(jax.random.fold_in(jax.random.fold_in(splits[15], part), 71), part),
        "mix_gain": jnp.clip(1.0 + 0.18 * jax.random.normal(splits[1], (D,), jnp.float32), 0.1, 1.9),
        "value_proj": normal_values(splits[2], (D, CA), D ** -0.5, 0.125, ((0, 16), (1, 8))),
        "gate_proj": normal_values(splits[3], (D, CA), D ** -0.5, 0.125, ((0, 16), (1, 8))),
        "conv_taps": normal_values(splits[4], (KW, CA), KW ** -0.5, 1.0, ((1, 8),), jnp.float32),
        "chan_gain": jnp.clip(1.0 + 0.18 * jax.random.normal(splits[5], (CA,), jnp.float32), 0.1, 1.9),
        "chan_shift": normal_values(splits[6], (CA,), 0.5, 3.0, (), jnp.float32),
        "mix_out": normal_values(splits[7], (CA, D), CA ** -0.5, 0.1875, ((0, 16), (1, 8))),
        "mlp_gain": jnp.clip(1.0 + 0.18 * jax.random.normal(splits[8], (D,), jnp.float32), 0.1, 1.9),
        "mlp_gate": normal_values(splits[9], (D, FF), D ** -0.5, 0.125, ((0, 16), (1, 8))),
        "mlp_up": normal_values(splits[10], (D, FF), D ** -0.5, 0.125, ((0, 16), (1, 8))),
        "gate_taps": normal_values(splits[11], (FKW, FF), FKW ** -0.5, 3.5, ((1, 8),), jnp.float32),
        "up_taps": normal_values(splits[12], (FKW, FF), FKW ** -0.5, 3.5, ((1, 8),), jnp.float32),
        "mlp_down": normal_values(splits[13], (FF, D), FF ** -0.5, 0.078125, ((0, 8), (1, 16))),
        "final_gain": jnp.clip(1.0 + 0.18 * jax.random.normal(splits[14], (D,), jnp.float32), 0.1, 1.9),
    }


def rms_scale(values, gain):
    return values * lax.rsqrt(lax.optimization_barrier(jnp.mean(values * values, axis=-1, keepdims=True)) + 1e-06) * gain

def along_sequences(values, taps, seq_len):
    width = taps.shape[0]
    half = (width - 1) // 2
    channels = values.shape[1]
    grouped = values.reshape(-1, seq_len, channels)
    padded = jnp.pad(grouped, ((0, 0), (half, width - 1 - half), (0, 0)))
    total = jnp.zeros_like(grouped)
    for offset in range(width):
        total = total + taps[offset] * padded[:, offset:offset + seq_len]
    return total.reshape(values.shape)

def reference(tokens, mix_gain, value_proj, gate_proj, conv_taps, chan_gain, chan_shift, mix_out, mlp_gain, mlp_gate, mlp_up, gate_taps, up_taps, mlp_down, final_gain):
    base = tokens.astype(jnp.float32)
    normed = rms_scale(base, mix_gain).astype(jnp.bfloat16)
    value = jnp.dot(normed, value_proj, preferred_element_type=jnp.float32)
    gate = jnp.dot(normed, gate_proj, preferred_element_type=jnp.float32)
    glu = value * jax.nn.sigmoid(gate)
    conv_out = along_sequences(glu, conv_taps, TOK_DEV).astype(jnp.bfloat16)
    conv_wide = conv_out.astype(jnp.float32)
    mean = lax.optimization_barrier(jnp.mean(conv_wide, axis=-1, keepdims=True))
    var = lax.optimization_barrier(jnp.mean(conv_wide * conv_wide, axis=-1, keepdims=True)) - mean * mean
    chan_norm = (conv_wide - mean) * lax.rsqrt(var + 1e-05) * chan_gain + chan_shift
    hidden_mix = jax.nn.silu(chan_norm).astype(jnp.bfloat16)
    mixed = (base + jnp.dot(hidden_mix, mix_out, preferred_element_type=jnp.float32)).astype(jnp.bfloat16)
    mixed_wide = mixed.astype(jnp.float32)
    normed_two = rms_scale(mixed_wide, mlp_gain).astype(jnp.bfloat16)
    gate_conv = along_sequences(jnp.dot(normed_two, mlp_gate, preferred_element_type=jnp.float32), gate_taps, TOK_DEV)
    up_conv = along_sequences(jnp.dot(normed_two, mlp_up, preferred_element_type=jnp.float32), up_taps, TOK_DEV)
    hidden_mlp = (jax.nn.silu(gate_conv) * up_conv).astype(jnp.bfloat16)
    mlp_out = jnp.zeros((tokens.shape[0], D), jnp.float32)
    for block in range(N_TP):
        lower = block * FF_BLOCK
        partial_sum = jnp.dot(hidden_mlp[:, lower:lower + FF_BLOCK], mlp_down[lower:lower + FF_BLOCK], preferred_element_type=jnp.float32)
        rounded = lax.optimization_barrier(partial_sum.astype(jnp.bfloat16))
        mlp_out = mlp_out + rounded.astype(jnp.float32)
    summed = mixed_wide + mlp_out
    return rms_scale(summed, final_gain).astype(jnp.bfloat16)
```

```python
import jax
import jax.numpy as jnp
from jax import lax
from jax.sharding import PartitionSpec as P


BF = jnp.bfloat16
F32 = jnp.float32


def shift(a, axis, by):
    n = lax.axis_size(axis)
    return lax.ppermute(a, axis, [(i, (i + by) % n) for i in range(n)])


def swap_core(a):
    n = lax.axis_size("tp")
    return lax.ppermute(a, "tp", [(i, i ^ 1) for i in range(n)])


def gather_fs(a):
    n = lax.axis_size("fs")
    q = n // 4
    me = lax.axis_index("fs")
    far = [a, shift(a, "fs", q), shift(a, "fs", 2 * q), shift(a, "fs", 3 * q)]
    quad = jnp.stack(far)
    out = jnp.zeros((n,) + a.shape, a.dtype)
    for by, piece in (
        (0, quad),
        (1, shift(quad, "fs", 1)),
        (-1, shift(quad, "fs", -1)),
        (2, shift(quad, "fs", 2)),
    ):
        for k in range(4):
            at = (me - by - k * q) % n
            out = lax.dynamic_update_slice(out, piece[k][None], (at, 0, 0))
    return out


def gather_tp(a):
    n = lax.axis_size("tp")
    me = lax.axis_index("tp")
    t, c = a.shape
    h = t // 2
    prev = shift(a, "tp", 2)
    nxt = shift(a, "tp", -2)
    opp_lo = shift(prev[:h], "tp", 2)
    opp_hi = shift(nxt[h:], "tp", -2)
    out = jnp.zeros((t, n * c), a.dtype)
    for piece, back, row in ((a, 0, 0), (prev, 2, 0), (nxt, -2, 0), (opp_lo, 4, 0), (opp_hi, 4, h)):
        src = (me - back) % n
        out = lax.dynamic_update_slice(out, piece, (row, src * c))
        out = lax.dynamic_update_slice(out, swap_core(piece), (row, (src ^ 1) * c))
    return out


def sum_tp_small(s):
    s = s + swap_core(s)
    return s + shift(s, "tp", 2) + shift(s, "tp", -2) + shift(s, "tp", 4)


def rms_scale(values, gain):
    return values * lax.rsqrt(jnp.mean(values * values, axis=-1, keepdims=True) + 1e-06) * gain


def along_sequence(values, taps):
    width = taps.shape[0]
    half = (width - 1) // 2
    length = values.shape[0]
    padded = jnp.pad(values, ((half, width - 1 - half), (0, 0)))
    total = jnp.zeros_like(values)
    for offset in range(width):
        total = total + taps[offset] * padded[offset : offset + length]
    return total


def local(
    tokens,
    mix_gain,
    value_proj,
    gate_proj,
    conv_taps,
    chan_gain,
    chan_shift,
    mix_out,
    mlp_gain,
    mlp_gate,
    mlp_up,
    gate_taps,
    up_taps,
    mlp_down,
    final_gain,
):
    width_tp = lax.axis_size("tp")
    width_fs = lax.axis_size("fs")
    me = lax.axis_index("tp")
    t, feat = tokens.shape
    hid = mlp_gate.shape[1]
    ca = value_proj.shape[1]

    big = jnp.concatenate([mlp_gate, mlp_up, mlp_down.T], axis=1)
    big = lax.all_gather(big, "fs", axis=0, tiled=True)

    whole = gather_tp(tokens)
    vg = gather_fs(jnp.concatenate([value_proj, gate_proj], axis=1))
    vg = vg.reshape(-1, 2 * ca)
    normed = rms_scale(whole.astype(F32), mix_gain).astype(BF)
    both = jnp.dot(normed, vg, preferred_element_type=F32)
    glu = both[:, :ca] * jax.nn.sigmoid(both[:, ca:])
    conv_out = along_sequence(glu, conv_taps).astype(BF)

    mix = gather_fs(mix_out).reshape(-1, feat)
    conv_all = gather_tp(conv_out).astype(F32)
    mean = jnp.mean(conv_all, axis=-1, keepdims=True)
    var = jnp.mean(conv_all * conv_all, axis=-1, keepdims=True) - mean * mean
    chan_norm = (conv_all - mean) * lax.rsqrt(var + 1e-05) * chan_gain + chan_shift
    hidden_mix = jax.nn.silu(chan_norm).astype(BF)
    mixer_result = jnp.dot(hidden_mix, mix, preferred_element_type=F32)
    mixed = (tokens.astype(F32) + mixer_result).astype(BF)
    whole_two = gather_tp(mixed)
    normed_two = rms_scale(whole_two.astype(F32), mlp_gain).astype(BF)

    gate_pre = jnp.dot(normed_two, big[:, :hid], preferred_element_type=F32)
    up_pre = jnp.dot(normed_two, big[:, hid : 2 * hid], preferred_element_type=F32)
    gate_conv = along_sequence(gate_pre, gate_taps)
    up_conv = along_sequence(up_pre, up_taps)
    hidden_mlp = (jax.nn.silu(gate_conv) * up_conv).astype(BF)

    core = me % 2
    down_t = big[:, 2 * hid :]

    def pair_sum(dx):
        x = (me // 2 + dx) % (width_tp // 2)
        rows = lax.dynamic_slice(down_t, (x * 2 * feat, 0), (2 * feat, hid))
        part = lax.dot_general(hidden_mlp, rows, (((1,), (1,)), ((), ())), preferred_element_type=F32)
        mine = jnp.where(core == 0, part[:, :feat], part[:, feat:])
        other = jnp.where(core == 0, part[:, feat:], part[:, :feat]).astype(BF)
        return mine + swap_core(other).astype(F32)

    h = t // 2
    far = pair_sum(2).astype(BF)
    via_next = shift(far[:h], "tp", 2)
    via_prev = shift(far[h:], "tp", -2)
    plus = pair_sum(1)
    plus = jnp.concatenate([plus[:h] + via_next.astype(F32), plus[h:]], axis=0).astype(BF)
    minus = pair_sum(-1)
    minus = jnp.concatenate([minus[:h], minus[h:] + via_prev.astype(F32)], axis=0).astype(BF)
    got_a = shift(plus, "tp", 2).astype(F32)
    got_b = shift(minus, "tp", -2).astype(F32)
    mlp_out = pair_sum(0) + got_a + got_b

    summed = mixed.astype(F32) + mlp_out
    squares = sum_tp_small(jnp.sum(summed * summed, axis=-1).reshape(-1, 128)).reshape(-1, 1)
    all_features = feat * width_tp
    layer_out = summed * lax.rsqrt(squares / all_features + 1e-06) * final_gain
    return layer_out.astype(BF)


def solution(mesh):
    return jax.shard_map(
        local,
        mesh=mesh,
        in_specs=(
            P(("grp", "fs"), "tp"),
            P(),
            P("fs", "tp"),
            P("fs", "tp"),
            P(None, "tp"),
            P(),
            P(),
            P("fs", "tp"),
            P(),
            P("fs", "tp"),
            P("fs", "tp"),
            P(None, "tp"),
            P(None, "tp"),
            P("tp", "fs"),
            P("tp"),
        ),
        out_specs=P(("grp", "fs"), "tp"),
        check_vma=False,
    )
```

```python
import functools

import jax
import jax.numpy as jnp
from jax import lax
from jax.experimental import pallas as pl
from jax.experimental.pallas import tpu as pltpu
from jax.sharding import PartitionSpec as P


BF = jnp.bfloat16
F32 = jnp.float32
LANES = 128
QUAD_BY = (0, 1, 2, -1)
MIB = 1024 * 1024


def shift(a, axis, by):
    n = lax.axis_size(axis)
    return lax.ppermute(a, axis, [(i, (i + by) % n) for i in range(n)])


def swap_core(a):
    n = lax.axis_size("tp")
    return lax.ppermute(a, "tp", [(i, i ^ 1) for i in range(n)])


def swap_group(a):
    n = lax.axis_size("grp")
    return lax.ppermute(a, "grp", [(i, i ^ 1) for i in range(n)])


def quads_fs(a):
    rows = a.shape[0] // 2
    a = lax.dynamic_slice_in_dim(a, (lax.axis_index("grp") % 2) * rows, rows, 0)
    q = lax.axis_size("fs") // 4
    quad = jnp.stack([a] + [shift(a, "fs", k * q) for k in (1, 2, 3)])
    quads = [quad] + [shift(quad, "fs", by) for by in QUAD_BY[1:]]
    return quads + [swap_group(piece) for piece in quads]


def pieces_tp(a):
    half = lax.axis_size("tp") // 2
    same = [a] + [shift(a, "tp", 2 * r) for r in range(1, half)]
    out = []
    for piece in same:
        out += [piece, swap_core(piece)]
    return out


def source(pos, me, n):
    return ((me // 2 - pos // 2) % (n // 2)) * 2 + (me % 2 + pos % 2) % 2


def position(src, me, n):
    return ((me // 2 - src // 2) % (n // 2)) * 2 + (me % 2 + src % 2) % 2


def place_quads(idx, quads, buf, n_tp, n_fs):
    rows = quads[0].shape[1]
    per = n_fs // n_tp
    for n, quad in enumerate(quads):
        part = idx[2] if n < 4 else 1 - idx[2]
        for k in range(4):
            f = (idx[1] + 2 * n_fs - QUAD_BY[n % 4] - k * (n_fs // 4)) % n_fs
            at = position(f // per, idx[0] + 2 * n_tp, n_tp) * (2 * per * rows) + (f % per) * 2 * rows + part * rows
            buf[pl.ds(pl.multiple_of(at, rows), rows), :] = quad[k]


def norm_rows(idx, parts, gain, at, store):
    n_tp = len(parts)
    width = parts[0].shape[1]
    total = 0.0
    for part in parts:
        x = part[at, :].astype(F32)
        total = total + x * x
    scale = lax.rsqrt(jnp.sum(total, axis=-1, keepdims=True) / (width * n_tp) + 1e-06)
    for p, part in enumerate(parts):
        src = source(p, idx[0] + 2 * n_tp, n_tp)
        store(p, src, (part[at, :].astype(F32) * scale * gain[src]).astype(BF))


def whole(a):
    return pl.BlockSpec(a.shape, lambda *i: (0,) * a.ndim)


def norm_in_kernel(n_tp, idx, *refs):
    parts, gain, out = refs[:n_tp], refs[n_tp], refs[n_tp + 1]
    width = parts[0].shape[1]
    chunk = 128

    def store_at(at):
        def store(p, src, value):
            out[at, p * width : (p + 1) * width] = value

        return store

    for i in range(parts[0].shape[0] // chunk):
        at = slice(i * chunk, (i + 1) * chunk)
        norm_rows(idx, parts, gain, at, store_at(at))


def norm_in(idx, toks, gain):
    n_tp = len(toks)
    t, width = toks[0].shape
    rows = 256
    return pl.pallas_call(
        functools.partial(norm_in_kernel, n_tp),
        grid=(t // rows,),
        in_specs=[pl.BlockSpec(memory_space=pltpu.SMEM)]
        + [pl.BlockSpec((rows, width), lambda i: (i, 0))] * n_tp
        + [whole(gain)],
        out_specs=pl.BlockSpec((rows, width * n_tp), lambda i: (i, 0)),
        out_shape=jax.ShapeDtypeStruct((t, width * n_tp), BF),
        compiler_params=pltpu.CompilerParams(vmem_limit_bytes=10 * MIB),
        name="norm_in",
    )(idx, *toks, gain)


def mixer_in_kernel(n_tp, n_fs, idx, normed, *refs):
    quads = refs[:8]
    taps, out, wbuf, gbuf = refs[8:]
    length, chans = out.shape
    pad = 16
    place_quads(idx, quads, wbuf, n_tp, n_fs)
    gbuf[0:pad, :] = jnp.zeros((pad, chans), F32)
    gbuf[pad + length :, :] = jnp.zeros((pad, chans), F32)
    both = jnp.dot(normed[...], wbuf[...], preferred_element_type=F32)
    gbuf[pad : pad + length, :] = both[:, :chans] * jax.nn.sigmoid(both[:, chans:])
    n_taps = taps.shape[0]
    first = pad - (n_taps - 1) // 2
    block = 64

    def body(i, carry):
        base = pl.multiple_of(i * block, block)
        acc = jnp.zeros((block, chans), F32)
        for s in range(8):
            win = gbuf[pl.ds(base + first + s, block + 24), :]
            for q in range(4):
                k = s + 8 * q
                if k < n_taps:
                    acc = acc + taps[k : k + 1, :] * win[8 * q : 8 * q + block]
        out[pl.ds(base, block), :] = acc.astype(BF)
        return carry

    lax.fori_loop(0, length // block, body, 0)


def mixer_in(idx, normed, quads, taps, n_tp, n_fs):
    t, feat = normed.shape
    chans = taps.shape[1]
    return pl.pallas_call(
        functools.partial(mixer_in_kernel, n_tp, n_fs),
        grid=(1,),
        in_specs=[pl.BlockSpec(memory_space=pltpu.SMEM), whole(normed)] + [whole(q) for q in quads] + [whole(taps)],
        out_specs=pl.BlockSpec((t, chans), lambda i: (0, 0)),
        out_shape=jax.ShapeDtypeStruct((t, chans), BF),
        scratch_shapes=[
            pltpu.VMEM((feat, 2 * chans), BF),
            pltpu.VMEM((t + 32, chans), F32),
        ],
        compiler_params=pltpu.CompilerParams(vmem_limit_bytes=16 * MIB),
        name="mixer_in",
    )(idx, normed, *quads, taps)


def mixer_out_kernel(n_tp, n_fs, idx, *refs):
    convs, quads = refs[:n_tp], refs[n_tp : n_tp + 8]
    gain, bias, resid, out, wbuf, hbuf = refs[n_tp + 8 :]

    @pl.when(pl.program_id(0) == 0)
    def _():
        place_quads(idx, quads, wbuf, n_tp, n_fs)

    chans = convs[0].shape[1]
    chunk = 128
    for i in range(convs[0].shape[0] // chunk):
        at = slice(i * chunk, (i + 1) * chunk)
        total, square = 0.0, 0.0
        for c in convs:
            x = c[at, :].astype(F32)
            total, square = total + x, square + x * x
        mean = jnp.sum(total, axis=-1, keepdims=True) / (chans * n_tp)
        square = jnp.sum(square, axis=-1, keepdims=True) / (chans * n_tp)
        scale = lax.rsqrt(square - mean * mean + 1e-05)
        for p, c in enumerate(convs):
            src = source(p, idx[0] + 2 * n_tp, n_tp)
            v = (c[at, :].astype(F32) - mean) * scale * gain[src] + bias[src]
            hbuf[at, p * chans : (p + 1) * chans] = (v * jax.nn.sigmoid(v)).astype(BF)
    result = jnp.dot(hbuf[...], wbuf[...], preferred_element_type=F32)
    out[...] = (resid[...].astype(F32) + result).astype(BF)


def mixer_out(idx, convs, quads, gain, bias, resid, n_fs):
    n_tp = len(convs)
    t, chans = convs[0].shape
    width = resid.shape[1]
    rows = 512
    return pl.pallas_call(
        functools.partial(mixer_out_kernel, n_tp, n_fs),
        grid=(t // rows,),
        in_specs=[pl.BlockSpec(memory_space=pltpu.SMEM)]
        + [pl.BlockSpec((rows, chans), lambda i: (i, 0))] * n_tp
        + [whole(q) for q in quads]
        + [whole(gain), whole(bias), pl.BlockSpec((rows, width), lambda i: (i, 0))],
        out_specs=pl.BlockSpec((rows, width), lambda i: (i, 0)),
        out_shape=jax.ShapeDtypeStruct((t, width), BF),
        scratch_shapes=[
            pltpu.VMEM((chans * n_tp, width), BF),
            pltpu.VMEM((rows, chans * n_tp), BF),
        ],
        compiler_params=pltpu.CompilerParams(vmem_limit_bytes=10 * MIB),
        name="mixer_out",
    )(idx, *convs, *quads, gain, bias, resid)


def feed_in_kernel(n_tp, idx, *refs):
    mixed = refs[:n_tp]
    gain, w, w_last, taps, out, nbuf, even, odd = refs[n_tp:]
    step = pl.program_id(0)
    last = pl.num_programs(0) - 1
    t, width = mixed[0].shape
    feat = width * n_tp
    chunk = 128

    @pl.when(step == 0)
    def _():
        for ybuf in (even, odd):
            ybuf[0:8, :] = jnp.zeros((8, 2 * LANES), F32)
            ybuf[8 + t :, :] = jnp.zeros((8, 2 * LANES), F32)

        def norm(i, carry):
            at = pl.ds(pl.multiple_of(i * chunk, chunk), chunk)

            def store(p, src, value):
                nbuf[at, pl.ds(pl.multiple_of(src * width, width), width)] = value

            norm_rows(idx, mixed, gain, at, store)
            return carry

        lax.fori_loop(0, t // chunk, norm, 0)

    def conv(ybuf, lo, hi, lanes):
        tap = taps[0]
        return (
            tap[0:1, lanes] * ybuf[lo + 7 : hi + 7, lanes]
            + tap[1:2, lanes] * ybuf[lo + 8 : hi + 8, lanes]
            + tap[2:3, lanes] * ybuf[lo + 9 : hi + 9, lanes]
        )

    def project(ybuf, lo, hi):
        block = w[...]
        both = jnp.concatenate(
            [block[:, :LANES].reshape(feat, LANES), block[:, LANES:].reshape(feat, LANES)], axis=1
        )
        ybuf[8 + lo : 8 + hi, :] = jnp.dot(nbuf[lo:hi, :], both, preferred_element_type=F32)

    def activate(ybuf, begin, end):
        for lo in range(begin, end, chunk):
            g = conv(ybuf, lo, lo + chunk, slice(0, LANES))
            u = conv(ybuf, lo, lo + chunk, slice(LANES, 2 * LANES))
            out[lo : lo + chunk, :] = (g * jax.nn.sigmoid(g) * u).astype(BF)

    for parity, now, before in ((0, even, odd), (1, odd, even)):

        @pl.when((step % 2 == parity) & (step < last - 1))
        def _():
            activate(before, 0, t)
            project(now, 0, t)

        @pl.when((step % 2 == parity) & (step == last - 1))
        def _():
            activate(before, 0, t)
            now[8 : 8 + t, :LANES] = jnp.dot(
                nbuf[...], w_last[...].reshape(feat, LANES), preferred_element_type=F32
            )

        @pl.when((step % 2 == parity) & (step == last))
        def _():
            for lo in range(0, t, chunk):
                g = conv(before, lo, lo + chunk, slice(0, LANES))
                h = g * jax.nn.sigmoid(g) * pltpu.roll(g, LANES // 2, 1)
                lane = lax.broadcasted_iota(jnp.int32, h.shape, 1)
                out[lo : lo + chunk, :] = jnp.where(lane < LANES // 2, h, 0.0).astype(BF)


def feed_in(idx, mixed, gain, big, taps, hid):
    n_tp = len(mixed)
    t, width = mixed[0].shape
    feat = width * n_tp
    full = hid // LANES
    n_fs, _, _ = big.shape
    return pl.pallas_call(
        functools.partial(feed_in_kernel, n_tp),
        grid=(full + 2,),
        in_specs=[pl.BlockSpec(memory_space=pltpu.SMEM)]
        + [whole(m) for m in mixed]
        + [
            whole(gain),
            pl.BlockSpec((n_fs, 2 * LANES, LANES), lambda j: (0, jnp.minimum(j, full - 1), 0)),
            pl.BlockSpec((n_fs, LANES, LANES), lambda j: (0, 2 * full, 0)),
            pl.BlockSpec((1,) + taps.shape[1:], lambda j: (jnp.maximum(j - 1, 0), 0, 0)),
        ],
        out_specs=pl.BlockSpec((t, LANES), lambda j: (0, jnp.maximum(j - 1, 0))),
        out_shape=jax.ShapeDtypeStruct((t, (full + 1) * LANES), BF),
        scratch_shapes=[
            pltpu.VMEM((t, feat), BF),
            pltpu.VMEM((t + 16, 2 * LANES), F32),
            pltpu.VMEM((t + 16, 2 * LANES), F32),
        ],
        compiler_params=pltpu.CompilerParams(vmem_limit_bytes=17 * MIB),
        name="feed_in",
    )(idx, *mixed, gain, big, big, taps)


def feed_out_kernel(n_out, n_add, idx, h, *refs):
    weights, add = refs[:n_out], refs[n_out : n_out + n_add]
    outs, wbuf = refs[n_out + n_add : -1], refs[-1]
    hid = weights[0].shape[1]

    @pl.when(pl.program_id(0) == 0)
    def _():
        for n, w in enumerate(weights):
            wbuf[n, :hid, :LANES] = w[0]
            wbuf[n, :hid, LANES:] = w[1]
            wbuf[n, hid:, :] = jnp.zeros((wbuf.shape[1] - hid, 2 * LANES), BF)

    for n, out in enumerate(outs):
        y = jnp.dot(h[...], wbuf[n], preferred_element_type=F32)
        if n_add:
            y = y + add[n][...].astype(F32)
        out[...] = y.astype(out.dtype)


def feed_out(idx, hidden, big, hid, turns, other, add, dtype):
    t, k = hidden.shape
    rows = 512
    n_fs, total, _ = big.shape
    n_x = n_fs // 4
    at = total // hid - 1

    def w_at(turn):
        def index(i, idx):
            return (2 * ((idx[0] // 2 + turn) % n_x) + (idx[0] % 2 + other) % 2, at, 0)

        return index

    block = pl.BlockSpec((rows, 2 * LANES), lambda i, idx: (i, 0))
    return pl.pallas_call(
        functools.partial(feed_out_kernel, len(turns), len(add)),
        grid_spec=pltpu.PrefetchScalarGridSpec(
            num_scalar_prefetch=1,
            grid=(t // rows,),
            in_specs=[pl.BlockSpec((rows, k), lambda i, idx: (i, 0))]
            + [pl.BlockSpec((2, hid, LANES), w_at(turn)) for turn in turns]
            + [block] * len(add),
            out_specs=[block] * len(turns),
            scratch_shapes=[pltpu.VMEM((len(turns), k, 2 * LANES), BF)],
        ),
        out_shape=[jax.ShapeDtypeStruct((t, 2 * LANES), dtype)] * len(turns),
        compiler_params=pltpu.CompilerParams(vmem_limit_bytes=10 * MIB),
        name="feed_out",
    )(idx, hidden, *([big] * len(turns)), *add)


def tiles(gate, up):
    cut = gate.shape[1] // LANES * LANES
    out = []
    for lo in range(0, cut, LANES):
        out += [gate[:, lo : lo + LANES], up[:, lo : lo + LANES]]
    return out + [jnp.concatenate([gate[:, cut:], up[:, cut:]], axis=1)]


def pack_taps(gate, up):
    parts = tiles(gate, up)
    parts.append(jnp.zeros_like(parts[-1]))
    return jnp.stack([jnp.concatenate(parts[n : n + 2], axis=1) for n in range(0, len(parts), 2)])


def sum_tp_small(s):
    s = s + swap_core(s)
    return s + sum(shift(s, "tp", 2 * r) for r in range(1, lax.axis_size("tp") // 2))


def local(
    tokens,
    mix_gain,
    value_proj,
    gate_proj,
    conv_taps,
    chan_gain,
    chan_shift,
    mix_out,
    mlp_gain,
    mlp_gate,
    mlp_up,
    gate_taps,
    up_taps,
    mlp_down,
    final_gain,
):
    n_tp = lax.axis_size("tp")
    n_fs = lax.axis_size("fs")
    idx = jnp.stack([lax.axis_index("tp"), lax.axis_index("fs"), lax.axis_index("grp") % 2]).astype(jnp.int32)
    _, feat = tokens.shape
    hid = mlp_gate.shape[1]
    rows_of = lambda v: v.reshape(n_tp, 1, -1)

    vg = quads_fs(jnp.concatenate([value_proj, gate_proj], axis=1))
    toks = pieces_tp(tokens)

    big = jnp.concatenate(tiles(mlp_gate, mlp_up) + [mlp_down], axis=0)
    big = pltpu.with_memory_space_constraint(lax.all_gather(big, "fs", axis=0), pltpu.HBM)

    normed = norm_in(idx, toks, rows_of(mix_gain))
    conv_out = mixer_in(idx, normed, vg, conv_taps, n_tp, n_fs)

    mix = quads_fs(mix_out)
    convs = pieces_tp(conv_out)
    mixed = mixer_out(idx, convs, mix, rows_of(chan_gain), rows_of(chan_shift), tokens, n_fs)

    taps = pack_taps(gate_taps, up_taps)
    hidden = feed_in(idx, pieces_tp(mixed), rows_of(mlp_gain), big, taps, hid)

    down = functools.partial(feed_out, idx, hidden, big, hid)
    (far,) = down((2,), 1, (), BF)
    far = swap_core(far)
    near = [swap_core(a) for a in down((1, 3, 0), 1, (), BF)]
    (far,) = down((2,), 0, (far,), BF)
    far = shift(far, "tp", 4)
    plus, minus = down((1, 3), 0, near[:2], BF)
    plus, minus = shift(plus, "tp", 2), shift(minus, "tp", -2)
    (here,) = down((0,), 0, near[2:], F32)

    summed = mixed.astype(F32) + here + far.astype(F32) + plus.astype(F32) + minus.astype(F32)
    squares = sum_tp_small(jnp.sum(summed * summed, axis=-1).reshape(-1, LANES)).reshape(-1, 1)
    layer_out = summed * lax.rsqrt(squares / (feat * n_tp) + 1e-06) * final_gain
    return layer_out.astype(BF)


def solution(mesh):
    return jax.shard_map(
        local,
        mesh=mesh,
        in_specs=(
            P(("grp", "fs"), "tp"),
            P(),
            P("fs", "tp"),
            P("fs", "tp"),
            P(None, "tp"),
            P(),
            P(),
            P("fs", "tp"),
            P(),
            P("fs", "tp"),
            P("fs", "tp"),
            P(None, "tp"),
            P(None, "tp"),
            P("tp", "fs"),
            P("tp"),
        ),
        out_specs=P(("grp", "fs"), "tp"),
        check_vma=False,
    )
```

```python
import functools

import jax
import jax.numpy as jnp
from jax import lax
from jax.experimental import pallas as pl
from jax.experimental.pallas import tpu as pltpu
from jax.sharding import PartitionSpec as P


BF = jnp.bfloat16
F32 = jnp.float32
LANES = 128
QUAD_BY = (0, 1, 2, -1)
MIB = 1024 * 1024
FEED_MIB = 18


def shift(a, axis, by):
    n = lax.axis_size(axis)
    return lax.ppermute(a, axis, [(i, (i + by) % n) for i in range(n)])


def swap_core(a):
    n = lax.axis_size("tp")
    return lax.ppermute(a, "tp", [(i, i ^ 1) for i in range(n)])


def swap_group(a):
    n = lax.axis_size("grp")
    return lax.ppermute(a, "grp", [(i, i ^ 1) for i in range(n)])


def half_rows(a):
    rows = a.shape[0] // 2
    return lax.dynamic_slice_in_dim(a, (lax.axis_index("grp") % 2) * rows, rows, 0)


def quads_fs(a):
    q = lax.axis_size("fs") // 4
    quad = jnp.stack([a] + [shift(a, "fs", k * q) for k in (1, 2, 3)])
    quads = [quad] + [shift(quad, "fs", by) for by in QUAD_BY[1:]]
    return quads + [swap_group(piece) for piece in quads]


def pieces_tp(a):
    half = lax.axis_size("tp") // 2
    same = [a] + [shift(a, "tp", 2 * r) for r in range(1, half)]
    out = []
    for piece in same:
        out += [piece, swap_core(piece)]
    return out


def source(pos, me, n):
    return ((me // 2 - pos // 2) % (n // 2)) * 2 + (me % 2 + pos % 2) % 2


def position(src, me, n):
    return ((me // 2 - src // 2) % (n // 2)) * 2 + (me % 2 + src % 2) % 2


def place_quads(idx, quads, buf, lo, rows, n_tp, n_fs):
    per = n_fs // n_tp
    for n, quad in enumerate(quads):
        part = idx[2] if n < 4 else 1 - idx[2]
        for k in range(4):
            f = (idx[1] + 2 * n_fs - QUAD_BY[n % 4] - k * (n_fs // 4)) % n_fs
            at = position(f // per, idx[0] + 2 * n_tp, n_tp) * (2 * per * rows) + (f % per) * 2 * rows + part * rows
            buf[pl.ds(pl.multiple_of(at, rows), rows), :] = quad[k, lo : lo + rows]


def norm_rows(idx, parts, gain, at, store):
    n_tp = len(parts)
    width = parts[0].shape[1]
    total = 0.0
    for part in parts:
        x = part[at, :].astype(F32)
        total = total + x * x
    scale = lax.rsqrt(jnp.sum(total, axis=-1, keepdims=True) / (width * n_tp) + 1e-06)
    for p, part in enumerate(parts):
        src = source(p, idx[0] + 2 * n_tp, n_tp)
        store(p, src, (part[at, :].astype(F32) * scale * gain[src]).astype(BF))


def whole(a):
    return pl.BlockSpec(a.shape, lambda *i: (0,) * a.ndim)


def norm_in_kernel(n_tp, idx, *refs):
    parts, gain, out = refs[:n_tp], refs[n_tp], refs[n_tp + 1]
    width = parts[0].shape[1]
    chunk = 128

    def store_at(at):
        def store(p, src, value):
            out[at, p * width : (p + 1) * width] = value

        return store

    for i in range(parts[0].shape[0] // chunk):
        at = slice(i * chunk, (i + 1) * chunk)
        norm_rows(idx, parts, gain, at, store_at(at))


def norm_in(idx, toks, gain):
    n_tp = len(toks)
    t, width = toks[0].shape
    rows = 256
    return pl.pallas_call(
        functools.partial(norm_in_kernel, n_tp),
        grid=(t // rows,),
        in_specs=[pl.BlockSpec(memory_space=pltpu.SMEM)]
        + [pl.BlockSpec((rows, width), lambda i: (i, 0))] * n_tp
        + [whole(gain)],
        out_specs=pl.BlockSpec((rows, width * n_tp), lambda i: (i, 0)),
        out_shape=jax.ShapeDtypeStruct((t, width * n_tp), BF),
        compiler_params=pltpu.CompilerParams(vmem_limit_bytes=10 * MIB),
        name="norm_in",
    )(idx, *toks, gain)


def mixer_in_kernel(n_tp, n_fs, idx, normed, *refs):
    quads = refs[:8]
    taps, out, wbuf, gbuf = refs[8:]
    length, chans = out.shape
    pad = 16
    place_quads(idx, quads, wbuf, 0, wbuf.shape[0] // (2 * n_fs), n_tp, n_fs)
    gbuf[0:pad, :] = jnp.zeros((pad, chans), F32)
    gbuf[pad + length :, :] = jnp.zeros((pad, chans), F32)
    both = jnp.dot(normed[...], wbuf[...], preferred_element_type=F32)
    gbuf[pad : pad + length, :] = both[:, :chans] * jax.nn.sigmoid(both[:, chans:])
    n_taps = taps.shape[0]
    first = pad - (n_taps - 1) // 2
    block = 64

    def body(i, carry):
        base = pl.multiple_of(i * block, block)
        acc = jnp.zeros((block, chans), F32)
        for s in range(8):
            win = gbuf[pl.ds(base + first + s, block + 24), :]
            for q in range(4):
                k = s + 8 * q
                if k < n_taps:
                    acc = acc + taps[k : k + 1, :] * win[8 * q : 8 * q + block]
        out[pl.ds(base, block), :] = acc.astype(BF)
        return carry

    lax.fori_loop(0, length // block, body, 0)


def mixer_in(idx, normed, quads, taps, n_tp, n_fs):
    t, feat = normed.shape
    chans = taps.shape[1]
    return pl.pallas_call(
        functools.partial(mixer_in_kernel, n_tp, n_fs),
        grid=(1,),
        in_specs=[pl.BlockSpec(memory_space=pltpu.SMEM), whole(normed)] + [whole(q) for q in quads] + [whole(taps)],
        out_specs=pl.BlockSpec((t, chans), lambda i: (0, 0)),
        out_shape=jax.ShapeDtypeStruct((t, chans), BF),
        scratch_shapes=[
            pltpu.VMEM((feat, 2 * chans), BF),
            pltpu.VMEM((t + 32, chans), F32),
        ],
        compiler_params=pltpu.CompilerParams(vmem_limit_bytes=16 * MIB),
        name="mixer_in",
    )(idx, normed, *quads, taps)


def mixer_out_kernel(n_tp, n_fs, idx, *refs):
    convs, quads = refs[:n_tp], refs[n_tp : n_tp + 8]
    gain, bias, resid, out, wbuf, hbuf = refs[n_tp + 8 :]

    @pl.when(pl.program_id(0) == 0)
    def _():
        rows = wbuf.shape[0] // (2 * n_fs)
        place_quads(idx, quads, wbuf, quads[0].shape[1] - rows, rows, n_tp, n_fs)

    chans = convs[0].shape[1]
    chunk = 128
    for i in range(convs[0].shape[0] // chunk):
        at = slice(i * chunk, (i + 1) * chunk)
        total, square = 0.0, 0.0
        for c in convs:
            x = c[at, :].astype(F32)
            total, square = total + x, square + x * x
        mean = jnp.sum(total, axis=-1, keepdims=True) / (chans * n_tp)
        square = jnp.sum(square, axis=-1, keepdims=True) / (chans * n_tp)
        scale = lax.rsqrt(square - mean * mean + 1e-05)
        for p, c in enumerate(convs):
            src = source(p, idx[0] + 2 * n_tp, n_tp)
            v = (c[at, :].astype(F32) - mean) * scale * gain[src] + bias[src]
            hbuf[at, p * chans : (p + 1) * chans] = (v * jax.nn.sigmoid(v)).astype(BF)
    result = jnp.dot(hbuf[...], wbuf[...], preferred_element_type=F32)
    out[...] = (resid[...].astype(F32) + result).astype(BF)


def mixer_out(idx, convs, quads, gain, bias, resid, n_fs):
    n_tp = len(convs)
    t, chans = convs[0].shape
    width = resid.shape[1]
    rows = 512
    return pl.pallas_call(
        functools.partial(mixer_out_kernel, n_tp, n_fs),
        grid=(t // rows,),
        in_specs=[pl.BlockSpec(memory_space=pltpu.SMEM)]
        + [pl.BlockSpec((rows, chans), lambda i: (i, 0))] * n_tp
        + [whole(q) for q in quads]
        + [whole(gain), whole(bias), pl.BlockSpec((rows, width), lambda i: (i, 0))],
        out_specs=pl.BlockSpec((rows, width), lambda i: (i, 0)),
        out_shape=jax.ShapeDtypeStruct((t, width), BF),
        scratch_shapes=[
            pltpu.VMEM((chans * n_tp, width), BF),
            pltpu.VMEM((rows, chans * n_tp), BF),
        ],
        compiler_params=pltpu.CompilerParams(vmem_limit_bytes=10 * MIB),
        name="mixer_out",
    )(idx, *convs, *quads, gain, bias, resid)


def feed_in_kernel(n_tp, begin, end, emit, idx, *refs):
    mixed = refs[:n_tp]
    gain, w, w_last, taps = refs[n_tp : n_tp + 4]
    rest = refs[n_tp + 4 :]
    if emit:
        down, (out, down_out) = rest[:2], rest[2:4]
        rest = rest[4:]
    else:
        out, rest = rest[0], rest[1:]
    nbuf, even, odd = rest
    step = pl.program_id(0)
    last = pl.num_programs(0) - 1
    _, width = mixed[0].shape
    feat = width * n_tp
    first = max(begin - 16, 0)
    rows = nbuf.shape[0]
    chunk = 128

    if emit:
        hid = down[0].shape[1]
        for core in range(2):
            down_out[0, core, :hid, :LANES] = down[core][0]
            down_out[0, core, :hid, LANES:] = down[core][1]
            down_out[0, core, hid:, :] = jnp.zeros((down_out.shape[2] - hid, 2 * LANES), BF)

    @pl.when(step == 0)
    def _():
        for ybuf in (even, odd):
            ybuf[0:8, :] = jnp.zeros((8, 2 * LANES), F32)
            ybuf[8 + rows :, :] = jnp.zeros((8, 2 * LANES), F32)

        def norm(at, size):
            src_rows = pl.ds(pl.multiple_of(first + at, 16), size)
            dst_rows = pl.ds(pl.multiple_of(at, 16), size)
            total = 0.0
            for part in mixed:
                x = part[src_rows, :].astype(F32)
                total = total + x * x
            scale = lax.rsqrt(jnp.sum(total, axis=-1, keepdims=True) / feat + 1e-06)
            for p, part in enumerate(mixed):
                src = source(p, idx[0] + 2 * n_tp, n_tp)
                cols = pl.ds(pl.multiple_of(src * width, width), width)
                nbuf[dst_rows, cols] = (part[src_rows, :].astype(F32) * scale * gain[src]).astype(BF)

        def body(i, carry):
            norm(i * chunk, chunk)
            return carry

        lax.fori_loop(0, rows // chunk, body, 0)
        if rows % chunk:
            norm(rows // chunk * chunk, rows % chunk)

    def conv(ybuf, lo, hi, lanes):
        tap = taps[0]
        at = 8 + begin - first
        return (
            tap[0:1, lanes] * ybuf[at + lo - 1 : at + hi - 1, lanes]
            + tap[1:2, lanes] * ybuf[at + lo : at + hi, lanes]
            + tap[2:3, lanes] * ybuf[at + lo + 1 : at + hi + 1, lanes]
        )

    for parity, now, before in ((0, even, odd), (1, odd, even)):

        @pl.when((step % 2 == parity) & (step < last))
        def _():
            for lo in range(0, end - begin, chunk):
                g = conv(before, lo, lo + chunk, slice(0, LANES))
                u = conv(before, lo, lo + chunk, slice(LANES, 2 * LANES))
                out[lo : lo + chunk, :] = (g * jax.nn.sigmoid(g) * u).astype(BF)

        @pl.when((step % 2 == parity) & (step < last - 1))
        def _():
            block = w[...]
            both = jnp.concatenate(
                [block[:, :LANES].reshape(feat, LANES), block[:, LANES:].reshape(feat, LANES)], axis=1
            )
            now[8 : 8 + rows, :] = jnp.dot(nbuf[...], both, preferred_element_type=F32)

        @pl.when((step % 2 == parity) & (step == last - 1))
        def _():
            now[8 : 8 + rows, :LANES] = jnp.dot(
                nbuf[...], w_last[...].reshape(feat, LANES), preferred_element_type=F32
            )

        @pl.when((step % 2 == parity) & (step == last))
        def _():
            for lo in range(0, end - begin, chunk):
                g = conv(before, lo, lo + chunk, slice(0, LANES))
                h = g * jax.nn.sigmoid(g) * pltpu.roll(g, LANES // 2, 1)
                lane = lax.broadcasted_iota(jnp.int32, h.shape, 1)
                out[lo : lo + chunk, :] = jnp.where(lane < LANES // 2, h, 0.0).astype(BF)


def feed_in(idx, mixed, gain, big, taps, hid, begin, end, emit):
    n_tp = len(mixed)
    t, width = mixed[0].shape
    feat = width * n_tp
    full = hid // LANES
    n_fs, total, _ = big.shape
    n_x = n_tp // 2
    rows = min(end + 16, t) - max(begin - 16, 0)
    k = (full + 1) * LANES
    fixed = lambda a: pl.BlockSpec(a.shape, lambda j, idx: (0,) * a.ndim)
    behind = lambda j: jnp.maximum(j - 1, 0)

    def down_at(other):
        def index(j, idx):
            x = (idx[0] // 2 + jnp.minimum(j, n_x - 1)) % n_x
            return (2 * x + (idx[0] % 2 + other) % 2, total // hid - 1, 0)

        return index

    out_specs = [pl.BlockSpec((end - begin, LANES), lambda j, idx: (0, behind(j)))]
    out_shape = [jax.ShapeDtypeStruct((end - begin, k), BF)]
    down_specs = []
    if emit:
        down_specs = [pl.BlockSpec((2, hid, LANES), down_at(other)) for other in range(2)]
        out_specs.append(pl.BlockSpec((1, 2, k, 2 * LANES), lambda j, idx: (jnp.minimum(j, n_x - 1), 0, 0, 0)))
        out_shape.append(jax.ShapeDtypeStruct((n_x, 2, k, 2 * LANES), BF))
    return pl.pallas_call(
        functools.partial(feed_in_kernel, n_tp, begin, end, emit),
        grid_spec=pltpu.PrefetchScalarGridSpec(
            num_scalar_prefetch=1,
            grid=(full + 2,),
            in_specs=[fixed(m) for m in mixed]
            + [
                fixed(gain),
                pl.BlockSpec((n_fs, 2 * LANES, LANES), lambda j, idx: (0, jnp.minimum(j, full - 1), 0)),
                pl.BlockSpec((n_fs, LANES, LANES), lambda j, idx: (0, 2 * full, 0)),
                pl.BlockSpec((1,) + taps.shape[1:], lambda j, idx: (behind(j), 0, 0)),
            ]
            + down_specs,
            out_specs=out_specs,
            scratch_shapes=[
                pltpu.VMEM((rows, feat), BF),
                pltpu.VMEM((rows + 16, 2 * LANES), F32),
                pltpu.VMEM((rows + 16, 2 * LANES), F32),
            ],
        ),
        out_shape=out_shape,
        compiler_params=pltpu.CompilerParams(vmem_limit_bytes=FEED_MIB * MIB),
        name="feed_in",
    )(idx, *mixed, gain, big, big, taps, *([big, big] if emit else []))


def give_kernel(h, down, out):
    for turn in range(out.shape[0]):
        out[turn] = jnp.dot(h[...], down[turn, 1], preferred_element_type=F32).astype(BF)


def keep_kernel(h, down, got, here, *sent):
    for turn, out in enumerate((here, *sent)):
        y = jnp.dot(h[...], down[turn, 0], preferred_element_type=F32) + got[turn].astype(F32)
        out[...] = y.astype(out.dtype)


def feed_out(h, down):
    t = h.shape[0]
    n_x, width = down.shape[0], down.shape[3]
    spec = pl.BlockSpec(memory_space=pltpu.VMEM)
    params = pltpu.CompilerParams(vmem_limit_bytes=6 * MIB)
    other = pl.pallas_call(
        give_kernel,
        in_specs=[spec] * 2,
        out_specs=spec,
        out_shape=jax.ShapeDtypeStruct((n_x, t, width), BF),
        compiler_params=params,
        name="give",
    )(h, down)
    return pl.pallas_call(
        keep_kernel,
        in_specs=[spec] * 3,
        out_specs=[spec] * n_x,
        out_shape=[jax.ShapeDtypeStruct((t, width), F32)] + [jax.ShapeDtypeStruct((t, width), BF)] * (n_x - 1),
        compiler_params=params,
        name="keep",
    )(h, down, swap_core(other))


def tiles(gate, up):
    cut = gate.shape[1] // LANES * LANES
    out = []
    for lo in range(0, cut, LANES):
        out += [gate[:, lo : lo + LANES], up[:, lo : lo + LANES]]
    return out + [jnp.concatenate([gate[:, cut:], up[:, cut:]], axis=1)]


def pack_kernel(gate, up, down, out):
    parts = tiles(gate, up)
    for n, part in enumerate(parts):
        out[n * part.shape[0] : (n + 1) * part.shape[0], :] = part
    out[len(parts) * parts[0].shape[0] :, :] = down[...]


def pack_weights(gate, up, down):
    rows = 2 * gate.shape[0] * gate.shape[1] // LANES + down.shape[0]
    spec = pl.BlockSpec(memory_space=pltpu.VMEM)
    return pl.pallas_call(
        pack_kernel,
        in_specs=[spec] * 3,
        out_specs=spec,
        out_shape=jax.ShapeDtypeStruct((rows, LANES), BF),
        compiler_params=pltpu.CompilerParams(vmem_limit_bytes=6 * MIB),
        name="pack",
    )(gate, up, down)


def pack_taps(gate, up):
    parts = tiles(gate, up)
    parts.append(jnp.zeros_like(parts[-1]))
    return jnp.stack([jnp.concatenate(parts[n : n + 2], axis=1) for n in range(0, len(parts), 2)])


def sum_tp_small(s):
    s = s + swap_core(s)
    return s + sum(shift(s, "tp", 2 * r) for r in range(1, lax.axis_size("tp") // 2))


def local(
    tokens,
    mix_gain,
    value_proj,
    gate_proj,
    conv_taps,
    chan_gain,
    chan_shift,
    mix_out,
    mlp_gain,
    mlp_gate,
    mlp_up,
    gate_taps,
    up_taps,
    mlp_down,
    final_gain,
):
    n_tp = lax.axis_size("tp")
    n_fs = lax.axis_size("fs")
    idx = jnp.stack([lax.axis_index("tp"), lax.axis_index("fs"), lax.axis_index("grp") % 2]).astype(jnp.int32)
    t, feat = tokens.shape
    hid = mlp_gate.shape[1]
    rows_of = lambda v: v.reshape(n_tp, 1, -1)

    value_gate = jnp.concatenate([value_proj, gate_proj], axis=1)
    quads = quads_fs(jnp.concatenate([half_rows(value_gate), half_rows(mix_out)], axis=0))
    toks = pieces_tp(tokens)

    big = pack_weights(mlp_gate, mlp_up, mlp_down)
    big = pltpu.with_memory_space_constraint(lax.all_gather(big, "fs", axis=0), pltpu.HBM)

    normed = norm_in(idx, toks, rows_of(mix_gain))
    conv_out = mixer_in(idx, normed, quads, conv_taps, n_tp, n_fs)
    convs = pieces_tp(conv_out)
    mixed = mixer_out(idx, convs, quads, rows_of(chan_gain), rows_of(chan_shift), tokens, n_fs)
    pieces = [pltpu.with_memory_space_constraint(p, pltpu.VMEM) for p in pieces_tp(mixed)]

    taps = pack_taps(gate_taps, up_taps)
    summed, down = [], None
    for begin in range(0, t, t // 2):
        end = begin + t // 2
        outs = feed_in(idx, pieces, rows_of(mlp_gain), big, taps, hid, begin, end, down is None)
        if down is None:
            down = outs[1]
        here, *sent = feed_out(outs[0], down)
        got = [shift(sent[r - 1], "tp", 2 * r) for r in range(len(sent), 0, -1)]
        total = mixed[begin:end].astype(F32) + here
        for part in got:
            total = total + part.astype(F32)
        summed.append(total)

    summed = jnp.concatenate(summed, axis=0)
    squares = sum_tp_small(jnp.sum(summed * summed, axis=-1).reshape(-1, LANES)).reshape(-1, 1)
    layer_out = summed * lax.rsqrt(squares / (feat * n_tp) + 1e-06) * final_gain
    return layer_out.astype(BF)


def solution(mesh):
    return jax.shard_map(
        local,
        mesh=mesh,
        in_specs=(
            P(("grp", "fs"), "tp"),
            P(),
            P("fs", "tp"),
            P("fs", "tp"),
            P(None, "tp"),
            P(),
            P(),
            P("fs", "tp"),
            P(),
            P("fs", "tp"),
            P("fs", "tp"),
            P(None, "tp"),
            P(None, "tp"),
            P("tp", "fs"),
            P("tp"),
        ),
        out_specs=P(("grp", "fs"), "tp"),
        check_vma=False,
    )
```

```python
import functools

import jax
import jax.numpy as jnp
from jax import lax
from jax.experimental import pallas as pl
from jax.experimental.pallas import tpu as pltpu
from jax.sharding import PartitionSpec as P


BF = jnp.bfloat16
F32 = jnp.float32
LANES = 128
QUAD_BY = (0, 1, 2, -1)
MIB = 1024 * 1024
FEED_MIB = 20
W_PARTS = 4


def shift(a, axis, by):
    n = lax.axis_size(axis)
    return lax.ppermute(a, axis, [(i, (i + by) % n) for i in range(n)])


def swap_core(a):
    n = lax.axis_size("tp")
    return lax.ppermute(a, "tp", [(i, i ^ 1) for i in range(n)])


def swap_group(a):
    n = lax.axis_size("grp")
    return lax.ppermute(a, "grp", [(i, i ^ 1) for i in range(n)])


def half_rows(a):
    rows = a.shape[0] // 2
    return lax.dynamic_slice_in_dim(a, (lax.axis_index("grp") % 2) * rows, rows, 0)


def quads_fs(a):
    q = lax.axis_size("fs") // 4
    quad = jnp.stack([a] + [shift(a, "fs", k * q) for k in (1, 2, 3)])
    quads = [quad] + [shift(quad, "fs", by) for by in QUAD_BY[1:]]
    return quads + [swap_group(piece) for piece in quads]


def pieces_tp(a):
    half = lax.axis_size("tp") // 2
    same = [a] + [shift(a, "tp", 2 * r) for r in range(1, half)]
    out = []
    for piece in same:
        out += [piece, swap_core(piece)]
    return out


def source(pos, me, n):
    return ((me // 2 - pos // 2) % (n // 2)) * 2 + (me % 2 + pos % 2) % 2


def position(src, me, n):
    return ((me // 2 - src // 2) % (n // 2)) * 2 + (me % 2 + src % 2) % 2


def place_quads(idx, quads, buf, lo, rows, n_tp, n_fs):
    per = n_fs // n_tp
    for n, quad in enumerate(quads):
        part = idx[2] if n < 4 else 1 - idx[2]
        for k in range(4):
            f = (idx[1] + 2 * n_fs - QUAD_BY[n % 4] - k * (n_fs // 4)) % n_fs
            at = position(f // per, idx[0] + 2 * n_tp, n_tp) * (2 * per * rows) + (f % per) * 2 * rows + part * rows
            buf[pl.ds(pl.multiple_of(at, rows), rows), :] = quad[k, lo : lo + rows]


def norm_rows(idx, parts, gain, at, store):
    n_tp = len(parts)
    width = parts[0].shape[1]
    total = 0.0
    for part in parts:
        x = part[at, :].astype(F32)
        total = total + x * x
    scale = lax.rsqrt(jnp.sum(total, axis=-1, keepdims=True) / (width * n_tp) + 1e-06)
    for p, part in enumerate(parts):
        src = source(p, idx[0] + 2 * n_tp, n_tp)
        store(p, src, (part[at, :].astype(F32) * scale * gain[src]).astype(BF))


def whole(a):
    return pl.BlockSpec(a.shape, lambda *i: (0,) * a.ndim)


def norm_in_kernel(n_tp, idx, *refs):
    parts, gain, out = refs[:n_tp], refs[n_tp], refs[n_tp + 1]
    width = parts[0].shape[1]
    chunk = 128

    def store_at(at):
        def store(p, src, value):
            out[at, p * width : (p + 1) * width] = value

        return store

    for i in range(parts[0].shape[0] // chunk):
        at = slice(i * chunk, (i + 1) * chunk)
        norm_rows(idx, parts, gain, at, store_at(at))


def norm_in(idx, toks, gain):
    n_tp = len(toks)
    t, width = toks[0].shape
    rows = 256
    return pl.pallas_call(
        functools.partial(norm_in_kernel, n_tp),
        grid=(t // rows,),
        in_specs=[pl.BlockSpec(memory_space=pltpu.SMEM)]
        + [pl.BlockSpec((rows, width), lambda i: (i, 0))] * n_tp
        + [whole(gain)],
        out_specs=pl.BlockSpec((rows, width * n_tp), lambda i: (i, 0)),
        out_shape=jax.ShapeDtypeStruct((t, width * n_tp), BF),
        compiler_params=pltpu.CompilerParams(vmem_limit_bytes=10 * MIB),
        name="norm_in",
    )(idx, *toks, gain)


def mixer_in_kernel(n_tp, n_fs, idx, normed, *refs):
    quads = refs[:8]
    taps, out, wbuf, gbuf = refs[8:]
    length, chans = out.shape
    pad = 16
    place_quads(idx, quads, wbuf, 0, wbuf.shape[0] // (2 * n_fs), n_tp, n_fs)
    gbuf[0:pad, :] = jnp.zeros((pad, chans), F32)
    gbuf[pad + length :, :] = jnp.zeros((pad, chans), F32)
    both = jnp.dot(normed[...], wbuf[...], preferred_element_type=F32)
    gbuf[pad : pad + length, :] = both[:, :chans] * jax.nn.sigmoid(both[:, chans:])
    n_taps = taps.shape[0]
    first = pad - (n_taps - 1) // 2
    block = 64

    def body(i, carry):
        base = pl.multiple_of(i * block, block)
        acc = jnp.zeros((block, chans), F32)
        for s in range(8):
            win = gbuf[pl.ds(base + first + s, block + 24), :]
            for q in range(4):
                k = s + 8 * q
                if k < n_taps:
                    acc = acc + taps[k : k + 1, :] * win[8 * q : 8 * q + block]
        out[pl.ds(base, block), :] = acc.astype(BF)
        return carry

    lax.fori_loop(0, length // block, body, 0)


def mixer_in(idx, normed, quads, taps, n_tp, n_fs):
    t, feat = normed.shape
    chans = taps.shape[1]
    return pl.pallas_call(
        functools.partial(mixer_in_kernel, n_tp, n_fs),
        grid=(1,),
        in_specs=[pl.BlockSpec(memory_space=pltpu.SMEM), whole(normed)] + [whole(q) for q in quads] + [whole(taps)],
        out_specs=pl.BlockSpec((t, chans), lambda i: (0, 0)),
        out_shape=jax.ShapeDtypeStruct((t, chans), BF),
        scratch_shapes=[
            pltpu.VMEM((feat, 2 * chans), BF),
            pltpu.VMEM((t + 32, chans), F32),
        ],
        compiler_params=pltpu.CompilerParams(vmem_limit_bytes=16 * MIB),
        name="mixer_in",
    )(idx, normed, *quads, taps)


def mixer_out_kernel(n_tp, n_fs, idx, *refs):
    convs, quads = refs[:n_tp], refs[n_tp : n_tp + 8]
    gain, bias, resid, out, wbuf, hbuf = refs[n_tp + 8 :]

    @pl.when(pl.program_id(0) == 0)
    def _():
        rows = wbuf.shape[0] // (2 * n_fs)
        place_quads(idx, quads, wbuf, quads[0].shape[1] - rows, rows, n_tp, n_fs)

    chans = convs[0].shape[1]
    chunk = 128
    for i in range(convs[0].shape[0] // chunk):
        at = slice(i * chunk, (i + 1) * chunk)
        total, square = 0.0, 0.0
        for c in convs:
            x = c[at, :].astype(F32)
            total, square = total + x, square + x * x
        mean = jnp.sum(total, axis=-1, keepdims=True) / (chans * n_tp)
        square = jnp.sum(square, axis=-1, keepdims=True) / (chans * n_tp)
        scale = lax.rsqrt(square - mean * mean + 1e-05)
        for p, c in enumerate(convs):
            src = source(p, idx[0] + 2 * n_tp, n_tp)
            v = (c[at, :].astype(F32) - mean) * scale * gain[src] + bias[src]
            hbuf[at, p * chans : (p + 1) * chans] = (v * jax.nn.sigmoid(v)).astype(BF)
    result = jnp.dot(hbuf[...], wbuf[...], preferred_element_type=F32)
    out[...] = (resid[...].astype(F32) + result).astype(BF)


def mixer_out(idx, convs, quads, gain, bias, resid, n_fs):
    n_tp = len(convs)
    t, chans = convs[0].shape
    width = resid.shape[1]
    rows = 512
    return pl.pallas_call(
        functools.partial(mixer_out_kernel, n_tp, n_fs),
        grid=(t // rows,),
        in_specs=[pl.BlockSpec(memory_space=pltpu.SMEM)]
        + [pl.BlockSpec((rows, chans), lambda i: (i, 0))] * n_tp
        + [whole(q) for q in quads]
        + [whole(gain), whole(bias), pl.BlockSpec((rows, width), lambda i: (i, 0))],
        out_specs=pl.BlockSpec((rows, width), lambda i: (i, 0)),
        out_shape=jax.ShapeDtypeStruct((t, width), BF),
        scratch_shapes=[
            pltpu.VMEM((chans * n_tp, width), BF),
            pltpu.VMEM((rows, chans * n_tp), BF),
        ],
        compiler_params=pltpu.CompilerParams(vmem_limit_bytes=10 * MIB),
        name="mixer_out",
    )(idx, *convs, *quads, gain, bias, resid)


def feed_in_kernel(n_tp, begin, end, emit, idx, *refs):
    mixed = refs[:n_tp]
    gain, w_last, taps = refs[n_tp : n_tp + 3]
    rest = refs[n_tp + 3 :]
    if emit:
        parts, down = rest[:W_PARTS], rest[W_PARTS : W_PARTS + 2]
        out, w_out, down_out, nbuf, even, odd = rest[W_PARTS + 2 :]
    else:
        w, out, nbuf, even, odd = rest
    step = pl.program_id(0)
    last = pl.num_programs(0) - 1
    _, width = mixed[0].shape
    feat = width * n_tp
    first = max(begin - 16, 0)
    rows = nbuf.shape[0]
    chunk = 128

    if emit:
        hid = down[0].shape[1]
        for core in range(2):
            down_out[0, core, :hid, :LANES] = down[core][0]
            down_out[0, core, :hid, LANES:] = down[core][1]
            down_out[0, core, hid:, :] = jnp.zeros((down_out.shape[2] - hid, 2 * LANES), BF)
        size = feat // W_PARTS
        for n, part in enumerate(parts):
            w_out[0, n * size : (n + 1) * size, :LANES] = part[:, :LANES].reshape(size, LANES)
            w_out[0, n * size : (n + 1) * size, LANES:] = part[:, LANES:].reshape(size, LANES)
        w = w_out

    @pl.when(step == 0)
    def _():
        for ybuf in (even, odd):
            ybuf[0:8, :] = jnp.zeros((8, 2 * LANES), F32)
            ybuf[8 + rows :, :] = jnp.zeros((8, 2 * LANES), F32)

        def norm(at, size):
            src_rows = pl.ds(pl.multiple_of(first + at, 16), size)
            dst_rows = pl.ds(pl.multiple_of(at, 16), size)
            total = 0.0
            for part in mixed:
                x = part[src_rows, :].astype(F32)
                total = total + x * x
            scale = lax.rsqrt(jnp.sum(total, axis=-1, keepdims=True) / feat + 1e-06)
            for p, part in enumerate(mixed):
                src = source(p, idx[0] + 2 * n_tp, n_tp)
                cols = pl.ds(pl.multiple_of(src * width, width), width)
                nbuf[dst_rows, cols] = (part[src_rows, :].astype(F32) * scale * gain[src]).astype(BF)

        def body(i, carry):
            norm(i * chunk, chunk)
            return carry

        lax.fori_loop(0, rows // chunk, body, 0)
        if rows % chunk:
            norm(rows // chunk * chunk, rows % chunk)

    def conv(ybuf, lo, hi, lanes):
        tap = taps[0]
        at = 8 + begin - first
        return (
            tap[0:1, lanes] * ybuf[at + lo - 1 : at + hi - 1, lanes]
            + tap[1:2, lanes] * ybuf[at + lo : at + hi, lanes]
            + tap[2:3, lanes] * ybuf[at + lo + 1 : at + hi + 1, lanes]
        )

    def activate(ybuf):
        for lo in range(0, end - begin, chunk):
            g = conv(ybuf, lo, lo + chunk, slice(0, LANES))
            u = conv(ybuf, lo, lo + chunk, slice(LANES, 2 * LANES))
            out[lo : lo + chunk, :] = (g * jax.nn.sigmoid(g) * u).astype(BF)

    for parity, now, before in ((0, even, odd), (1, odd, even)):

        @pl.when((step % 2 == parity) & (step < last - 1))
        def _():
            activate(before)
            now[8 : 8 + rows, :] = jnp.dot(nbuf[...], w[0], preferred_element_type=F32)

        @pl.when((step % 2 == parity) & (step == last - 1))
        def _():
            activate(before)
            now[8 : 8 + rows, :LANES] = jnp.dot(
                nbuf[...], w_last[...].reshape(feat, LANES), preferred_element_type=F32
            )

        @pl.when((step % 2 == parity) & (step == last))
        def _():
            for lo in range(0, end - begin, chunk):
                g = conv(before, lo, lo + chunk, slice(0, LANES))
                h = g * jax.nn.sigmoid(g) * pltpu.roll(g, LANES // 2, 1)
                lane = lax.broadcasted_iota(jnp.int32, h.shape, 1)
                out[lo : lo + chunk, :] = jnp.where(lane < LANES // 2, h, 0.0).astype(BF)


def feed_in(idx, mixed, gain, big, taps, hid, begin, end, weights):
    n_tp = len(mixed)
    t, width = mixed[0].shape
    feat = width * n_tp
    full = hid // LANES
    n_fs, total, _ = big.shape
    n_x = n_tp // 2
    rows = min(end + 16, t) - max(begin - 16, 0)
    k = (full + 1) * LANES
    emit = weights is None
    fixed = lambda a: pl.BlockSpec(a.shape, lambda j, idx: (0,) * a.ndim)
    behind = lambda j: jnp.maximum(j - 1, 0)

    def part_at(n):
        return lambda j, idx: (n, jnp.minimum(j, full - 1), 0)

    def down_at(other):
        def index(j, idx):
            x = (idx[0] // 2 + jnp.minimum(j, n_x - 1)) % n_x
            return (2 * x + (idx[0] % 2 + other) % 2, total // hid - 1, 0)

        return index

    out_specs = [pl.BlockSpec((end - begin, LANES), lambda j, idx: (0, behind(j)))]
    out_shape = [jax.ShapeDtypeStruct((end - begin, k), BF)]
    w_spec = pl.BlockSpec((1, feat, 2 * LANES), lambda j, idx: (jnp.minimum(j, full - 1), 0, 0))
    if emit:
        w_specs = [pl.BlockSpec((n_fs // W_PARTS, 2 * LANES, LANES), part_at(n)) for n in range(W_PARTS)]
        w_specs += [pl.BlockSpec((2, hid, LANES), down_at(other)) for other in range(2)]
        w_args = [big] * (W_PARTS + 2)
        out_specs.append(w_spec)
        out_shape.append(jax.ShapeDtypeStruct((full, feat, 2 * LANES), BF))
        out_specs.append(pl.BlockSpec((1, 2, k, 2 * LANES), lambda j, idx: (jnp.minimum(j, n_x - 1), 0, 0, 0)))
        out_shape.append(jax.ShapeDtypeStruct((n_x, 2, k, 2 * LANES), BF))
    else:
        w_specs, w_args = [w_spec], [weights]
    return pl.pallas_call(
        functools.partial(feed_in_kernel, n_tp, begin, end, emit),
        grid_spec=pltpu.PrefetchScalarGridSpec(
            num_scalar_prefetch=1,
            grid=(full + 2,),
            in_specs=[fixed(m) for m in mixed]
            + [
                fixed(gain),
                pl.BlockSpec((n_fs, LANES, LANES), lambda j, idx: (0, 2 * full, 0)),
                pl.BlockSpec((1,) + taps.shape[1:], lambda j, idx: (behind(j), 0, 0)),
            ]
            + w_specs,
            out_specs=out_specs,
            scratch_shapes=[
                pltpu.VMEM((rows, feat), BF),
                pltpu.VMEM((rows + 16, 2 * LANES), F32),
                pltpu.VMEM((rows + 16, 2 * LANES), F32),
            ],
        ),
        out_shape=out_shape,
        compiler_params=pltpu.CompilerParams(vmem_limit_bytes=FEED_MIB * MIB),
        name="feed_in",
    )(idx, *mixed, gain, big, taps, *w_args)


def give_kernel(h, down, out):
    for turn in range(out.shape[0]):
        out[turn] = jnp.dot(h[...], down[turn, 1], preferred_element_type=F32).astype(BF)


def keep_kernel(h, down, got, here, *sent):
    for turn, out in enumerate((here, *sent)):
        y = jnp.dot(h[...], down[turn, 0], preferred_element_type=F32) + got[turn].astype(F32)
        out[...] = y.astype(out.dtype)


def feed_out(h, down):
    t = h.shape[0]
    n_x, width = down.shape[0], down.shape[3]
    spec = pl.BlockSpec(memory_space=pltpu.VMEM)
    params = pltpu.CompilerParams(vmem_limit_bytes=6 * MIB)
    other = pl.pallas_call(
        give_kernel,
        in_specs=[spec] * 2,
        out_specs=spec,
        out_shape=jax.ShapeDtypeStruct((n_x, t, width), BF),
        compiler_params=params,
        name="give",
    )(h, down)
    return pl.pallas_call(
        keep_kernel,
        in_specs=[spec] * 3,
        out_specs=[spec] * n_x,
        out_shape=[jax.ShapeDtypeStruct((t, width), F32)] + [jax.ShapeDtypeStruct((t, width), BF)] * (n_x - 1),
        compiler_params=params,
        name="keep",
    )(h, down, swap_core(other))


def tiles(gate, up):
    cut = gate.shape[1] // LANES * LANES
    out = []
    for lo in range(0, cut, LANES):
        out += [gate[:, lo : lo + LANES], up[:, lo : lo + LANES]]
    return out + [jnp.concatenate([gate[:, cut:], up[:, cut:]], axis=1)]


def pack_kernel(gate, up, down, gate_taps, up_taps, out, taps):
    parts = tiles(gate[...].T, up[...].T)
    for n, part in enumerate(parts):
        out[n * part.shape[0] : (n + 1) * part.shape[0], :] = part
    out[len(parts) * parts[0].shape[0] :, :] = down[...]
    parts = tiles(gate_taps, up_taps)
    parts.append(jnp.zeros_like(parts[-1]))
    for n in range(taps.shape[0]):
        taps[n] = jnp.concatenate(parts[2 * n : 2 * n + 2], axis=1)


def pack_weights(gate, up, down, gate_taps, up_taps):
    rows = 2 * gate.shape[0] * gate.shape[1] // LANES + down.shape[0]
    pairs = gate.shape[1] // LANES + 1
    spec = pl.BlockSpec(memory_space=pltpu.VMEM)
    return pl.pallas_call(
        pack_kernel,
        in_specs=[spec] * 5,
        out_specs=[spec] * 2,
        out_shape=[
            jax.ShapeDtypeStruct((rows, LANES), BF),
            jax.ShapeDtypeStruct((pairs, gate_taps.shape[0], 2 * LANES), F32),
        ],
        compiler_params=pltpu.CompilerParams(vmem_limit_bytes=6 * MIB),
        name="pack",
    )(gate.T, up.T, down, gate_taps, up_taps)


def sum_tp_small(s):
    s = s + swap_core(s)
    return s + sum(shift(s, "tp", 2 * r) for r in range(1, lax.axis_size("tp") // 2))


def local(
    tokens,
    mix_gain,
    value_proj,
    gate_proj,
    conv_taps,
    chan_gain,
    chan_shift,
    mix_out,
    mlp_gain,
    mlp_gate,
    mlp_up,
    gate_taps,
    up_taps,
    mlp_down,
    final_gain,
):
    n_tp = lax.axis_size("tp")
    n_fs = lax.axis_size("fs")
    idx = jnp.stack([lax.axis_index("tp"), lax.axis_index("fs"), lax.axis_index("grp") % 2]).astype(jnp.int32)
    t, feat = tokens.shape
    hid = mlp_gate.shape[1]
    rows_of = lambda v: v.reshape(n_tp, 1, -1)

    value_gate = jnp.concatenate([value_proj, gate_proj], axis=1)
    quads = quads_fs(jnp.concatenate([half_rows(value_gate), half_rows(mix_out)], axis=0))
    toks = pieces_tp(tokens)

    big, taps = pack_weights(mlp_gate, mlp_up, mlp_down, gate_taps, up_taps)
    big = pltpu.with_memory_space_constraint(lax.all_gather(big, "fs", axis=0), pltpu.HBM)

    normed = norm_in(idx, toks, rows_of(mix_gain))
    conv_out = mixer_in(idx, normed, quads, conv_taps, n_tp, n_fs)
    convs = pieces_tp(conv_out)
    mixed = mixer_out(idx, convs, quads, rows_of(chan_gain), rows_of(chan_shift), tokens, n_fs)
    pieces = [pltpu.with_memory_space_constraint(p, pltpu.VMEM) for p in pieces_tp(mixed)]

    summed, down, weights = [], None, None
    for begin in range(0, t, t // 2):
        end = begin + t // 2
        outs = feed_in(idx, pieces, rows_of(mlp_gain), big, taps, hid, begin, end, weights)
        if weights is None:
            weights, down = outs[1:]
        here, *sent = feed_out(outs[0], down)
        got = [shift(sent[r - 1], "tp", 2 * r) for r in range(len(sent), 0, -1)]
        total = mixed[begin:end].astype(F32) + here
        for part in got:
            total = total + part.astype(F32)
        summed.append(total)

    summed = jnp.concatenate(summed, axis=0)
    squares = sum_tp_small(jnp.sum(summed * summed, axis=-1).reshape(-1, LANES)).reshape(-1, 1)
    layer_out = summed * lax.rsqrt(squares / (feat * n_tp) + 1e-06) * final_gain
    return layer_out.astype(BF)


def solution(mesh):
    return jax.shard_map(
        local,
        mesh=mesh,
        in_specs=(
            P(("grp", "fs"), "tp"),
            P(),
            P("fs", "tp"),
            P("fs", "tp"),
            P(None, "tp"),
            P(),
            P(),
            P("fs", "tp"),
            P(),
            P("fs", "tp"),
            P("fs", "tp"),
            P(None, "tp"),
            P(None, "tp"),
            P("tp", "fs"),
            P("tp"),
        ),
        out_specs=P(("grp", "fs"), "tp"),
        check_vma=False,
    )
```

```python
import functools

import jax
import jax.numpy as jnp
from jax import lax
from jax.experimental import pallas as pl
from jax.experimental.pallas import tpu as pltpu
from jax.sharding import PartitionSpec as P


BF = jnp.bfloat16
F32 = jnp.float32
LANES = 128
QUAD_BY = (0, 1, 2, -1)
MIB = 1024 * 1024
FEED_MIB = 16
W_PARTS = 4


def shift(a, axis, by):
    n = lax.axis_size(axis)
    return lax.ppermute(a, axis, [(i, (i + by) % n) for i in range(n)])


def swap_core(a):
    n = lax.axis_size("tp")
    return lax.ppermute(a, "tp", [(i, i ^ 1) for i in range(n)])


def swap_group(a):
    n = lax.axis_size("grp")
    return lax.ppermute(a, "grp", [(i, i ^ 1) for i in range(n)])


def half_rows(a):
    rows = a.shape[0] // 2
    return lax.dynamic_slice_in_dim(a, (lax.axis_index("grp") % 2) * rows, rows, 0)


def quads_fs(a):
    q = lax.axis_size("fs") // 4
    quad = jnp.stack([a] + [shift(a, "fs", k * q) for k in (1, 2, 3)])
    quads = [quad] + [shift(quad, "fs", by) for by in QUAD_BY[1:]]
    return quads + [swap_group(piece) for piece in quads]


def pieces_tp(a):
    half = lax.axis_size("tp") // 2
    same = [a] + [shift(a, "tp", 2 * r) for r in range(1, half)]
    out = []
    for piece in same:
        out += [piece, swap_core(piece)]
    return out


def source(pos, me, n):
    return ((me // 2 - pos // 2) % (n // 2)) * 2 + (me % 2 + pos % 2) % 2


def position(src, me, n):
    return ((me // 2 - src // 2) % (n // 2)) * 2 + (me % 2 + src % 2) % 2


def place_quads(idx, quads, buf, lo, rows, n_tp, n_fs):
    per = n_fs // n_tp
    for n, quad in enumerate(quads):
        part = idx[2] if n < 4 else 1 - idx[2]
        for k in range(4):
            f = (idx[1] + 2 * n_fs - QUAD_BY[n % 4] - k * (n_fs // 4)) % n_fs
            at = position(f // per, idx[0] + 2 * n_tp, n_tp) * (2 * per * rows) + (f % per) * 2 * rows + part * rows
            buf[pl.ds(pl.multiple_of(at, rows), rows), :] = quad[k, lo : lo + rows]


def norm_rows(idx, parts, gain, at, store):
    n_tp = len(parts)
    width = parts[0].shape[1]
    total = 0.0
    for part in parts:
        x = part[at, :].astype(F32)
        total = total + x * x
    scale = lax.rsqrt(jnp.sum(total, axis=-1, keepdims=True) / (width * n_tp) + 1e-06)
    for p, part in enumerate(parts):
        src = source(p, idx[0] + 2 * n_tp, n_tp)
        store(p, src, (part[at, :].astype(F32) * scale * gain[src]).astype(BF))


def whole(a):
    return pl.BlockSpec(a.shape, lambda *i: (0,) * a.ndim)


def norm_in_kernel(n_tp, absolute, idx, *refs):
    parts, gain, out = refs[:n_tp], refs[n_tp], refs[n_tp + 1]
    width = parts[0].shape[1]
    chunk = 128

    def store_at(at):
        def store(p, src, value):
            if absolute:
                out[at, pl.ds(pl.multiple_of(src * width, width), width)] = value
            else:
                out[at, p * width : (p + 1) * width] = value

        return store

    for i in range(parts[0].shape[0] // chunk):
        at = slice(i * chunk, (i + 1) * chunk)
        norm_rows(idx, parts, gain, at, store_at(at))


def norm_in(idx, toks, gain, absolute):
    n_tp = len(toks)
    t, width = toks[0].shape
    rows = 256
    return pl.pallas_call(
        functools.partial(norm_in_kernel, n_tp, absolute),
        grid=(t // rows,),
        in_specs=[pl.BlockSpec(memory_space=pltpu.SMEM)]
        + [pl.BlockSpec((rows, width), lambda i: (i, 0))] * n_tp
        + [whole(gain)],
        out_specs=pl.BlockSpec((rows, width * n_tp), lambda i: (i, 0)),
        out_shape=jax.ShapeDtypeStruct((t, width * n_tp), BF),
        compiler_params=pltpu.CompilerParams(vmem_limit_bytes=10 * MIB),
    )(idx, *toks, gain)


def mixer_in_kernel(n_tp, n_fs, idx, normed, *refs):
    quads = refs[:8]
    taps, out, wbuf, gbuf = refs[8:]
    length, chans = out.shape
    pad = 16
    place_quads(idx, quads, wbuf, 0, wbuf.shape[0] // (2 * n_fs), n_tp, n_fs)
    gbuf[0:pad, :] = jnp.zeros((pad, chans), F32)
    gbuf[pad + length :, :] = jnp.zeros((pad, chans), F32)
    both = jnp.dot(normed[...], wbuf[...], preferred_element_type=F32)
    gbuf[pad : pad + length, :] = both[:, :chans] * jax.nn.sigmoid(both[:, chans:])
    n_taps = taps.shape[0]
    first = pad - (n_taps - 1) // 2
    block = 64

    def body(i, carry):
        base = pl.multiple_of(i * block, block)
        acc = jnp.zeros((block, chans), F32)
        for s in range(8):
            win = gbuf[pl.ds(base + first + s, block + 24), :]
            for q in range(4):
                k = s + 8 * q
                if k < n_taps:
                    acc = acc + taps[k : k + 1, :] * win[8 * q : 8 * q + block]
        out[pl.ds(base, block), :] = acc.astype(BF)
        return carry

    lax.fori_loop(0, length // block, body, 0)


def mixer_in(idx, normed, quads, taps, n_tp, n_fs):
    t, feat = normed.shape
    chans = taps.shape[1]
    return pl.pallas_call(
        functools.partial(mixer_in_kernel, n_tp, n_fs),
        grid=(1,),
        in_specs=[pl.BlockSpec(memory_space=pltpu.SMEM), whole(normed)] + [whole(q) for q in quads] + [whole(taps)],
        out_specs=pl.BlockSpec((t, chans), lambda i: (0, 0)),
        out_shape=jax.ShapeDtypeStruct((t, chans), BF),
        scratch_shapes=[
            pltpu.VMEM((feat, 2 * chans), BF),
            pltpu.VMEM((t + 32, chans), F32),
        ],
        compiler_params=pltpu.CompilerParams(vmem_limit_bytes=16 * MIB),
        name="mixer_in",
    )(idx, normed, *quads, taps)


def mixer_out_kernel(n_tp, n_fs, idx, *refs):
    convs, quads = refs[:n_tp], refs[n_tp : n_tp + 8]
    gain, bias, resid, out, wbuf, hbuf = refs[n_tp + 8 :]

    @pl.when(pl.program_id(0) == 0)
    def _():
        rows = wbuf.shape[0] // (2 * n_fs)
        place_quads(idx, quads, wbuf, quads[0].shape[1] - rows, rows, n_tp, n_fs)

    chans = convs[0].shape[1]
    chunk = 128
    for i in range(convs[0].shape[0] // chunk):
        at = slice(i * chunk, (i + 1) * chunk)
        total, square = 0.0, 0.0
        for c in convs:
            x = c[at, :].astype(F32)
            total, square = total + x, square + x * x
        mean = jnp.sum(total, axis=-1, keepdims=True) / (chans * n_tp)
        square = jnp.sum(square, axis=-1, keepdims=True) / (chans * n_tp)
        scale = lax.rsqrt(square - mean * mean + 1e-05)
        for p, c in enumerate(convs):
            src = source(p, idx[0] + 2 * n_tp, n_tp)
            v = (c[at, :].astype(F32) - mean) * scale * gain[src] + bias[src]
            hbuf[at, p * chans : (p + 1) * chans] = (v * jax.nn.sigmoid(v)).astype(BF)
    result = jnp.dot(hbuf[...], wbuf[...], preferred_element_type=F32)
    out[...] = (resid[...].astype(F32) + result).astype(BF)


def mixer_out(idx, convs, quads, gain, bias, resid, n_fs):
    n_tp = len(convs)
    t, chans = convs[0].shape
    width = resid.shape[1]
    rows = 512
    return pl.pallas_call(
        functools.partial(mixer_out_kernel, n_tp, n_fs),
        grid=(t // rows,),
        in_specs=[pl.BlockSpec(memory_space=pltpu.SMEM)]
        + [pl.BlockSpec((rows, chans), lambda i: (i, 0))] * n_tp
        + [whole(q) for q in quads]
        + [whole(gain), whole(bias), pl.BlockSpec((rows, width), lambda i: (i, 0))],
        out_specs=pl.BlockSpec((rows, width), lambda i: (i, 0)),
        out_shape=jax.ShapeDtypeStruct((t, width), BF),
        scratch_shapes=[
            pltpu.VMEM((chans * n_tp, width), BF),
            pltpu.VMEM((rows, chans * n_tp), BF),
        ],
        compiler_params=pltpu.CompilerParams(vmem_limit_bytes=10 * MIB),
        name="mixer_out",
    )(idx, *convs, *quads, gain, bias, resid)


def feed_in_kernel(idx, normed, w_last, taps, *refs):
    parts, down = refs[:W_PARTS], refs[W_PARTS : W_PARTS + 2]
    *outs, down_out, w, even, odd = refs[W_PARTS + 2 :]
    step = pl.program_id(0)
    last = pl.num_programs(0) - 1
    t, feat = normed.shape
    chunk = 128

    hid = down[0].shape[1]
    for core in range(2):
        down_out[0, core, :hid, :LANES] = down[core][0]
        down_out[0, core, :hid, LANES:] = down[core][1]
        down_out[0, core, hid:, :] = jnp.zeros((down_out.shape[2] - hid, 2 * LANES), BF)

    @pl.when(step == 0)
    def _():
        for ybuf in (even, odd):
            ybuf[0:8, :] = jnp.zeros((8, 2 * LANES), F32)
            ybuf[8 + t :, :] = jnp.zeros((8, 2 * LANES), F32)

    def conv(ybuf, lo, hi, lanes):
        tap = taps[0]
        return (
            tap[0:1, lanes] * ybuf[lo + 7 : hi + 7, lanes]
            + tap[1:2, lanes] * ybuf[lo + 8 : hi + 8, lanes]
            + tap[2:3, lanes] * ybuf[lo + 9 : hi + 9, lanes]
        )

    def store(lo, value):
        n, at = divmod(lo, outs[0].shape[0])
        outs[n][at : at + chunk, :] = value.astype(BF)

    def activate(ybuf):
        for lo in range(0, t, chunk):
            g = conv(ybuf, lo, lo + chunk, slice(0, LANES))
            u = conv(ybuf, lo, lo + chunk, slice(LANES, 2 * LANES))
            store(lo, g * jax.nn.sigmoid(g) * u)

    for parity, now, before in ((0, even, odd), (1, odd, even)):

        @pl.when((step % 2 == parity) & (step < last - 1))
        def _():
            size = feat // W_PARTS
            for n, part in enumerate(parts):
                w[n * size : (n + 1) * size, :LANES] = part[:, :LANES].reshape(size, LANES)
                w[n * size : (n + 1) * size, LANES:] = part[:, LANES:].reshape(size, LANES)
            activate(before)
            now[8 : 8 + t, :] = jnp.dot(normed[...], w[...], preferred_element_type=F32)

        @pl.when((step % 2 == parity) & (step == last - 1))
        def _():
            activate(before)
            now[8 : 8 + t, :LANES] = jnp.dot(
                normed[...], w_last[...].reshape(feat, LANES), preferred_element_type=F32
            )

        @pl.when((step % 2 == parity) & (step == last))
        def _():
            for lo in range(0, t, chunk):
                g = conv(before, lo, lo + chunk, slice(0, LANES))
                h = g * jax.nn.sigmoid(g) * pltpu.roll(g, LANES // 2, 1)
                lane = lax.broadcasted_iota(jnp.int32, h.shape, 1)
                store(lo, jnp.where(lane < LANES // 2, h, 0.0))


def feed_in(idx, normed, big, taps, hid, n_tp):
    t, feat = normed.shape
    full = hid // LANES
    n_fs, total, _ = big.shape
    n_x = n_tp // 2
    k = (full + 1) * LANES
    fixed = lambda a: pl.BlockSpec(a.shape, lambda j, idx: (0,) * a.ndim)
    behind = lambda j: jnp.maximum(j - 1, 0)

    def part_at(n):
        return lambda j, idx: (n, jnp.minimum(j, full - 1), 0)

    def down_at(other):
        def index(j, idx):
            x = (idx[0] // 2 + jnp.minimum(j, n_x - 1)) % n_x
            return (2 * x + (idx[0] % 2 + other) % 2, total // hid - 1, 0)

        return index

    return pl.pallas_call(
        feed_in_kernel,
        grid_spec=pltpu.PrefetchScalarGridSpec(
            num_scalar_prefetch=1,
            grid=(full + 2,),
            in_specs=[
                fixed(normed),
                pl.BlockSpec((n_fs, LANES, LANES), lambda j, idx: (0, 2 * full, 0)),
                pl.BlockSpec((1,) + taps.shape[1:], lambda j, idx: (behind(j), 0, 0)),
            ]
            + [pl.BlockSpec((n_fs // W_PARTS, 2 * LANES, LANES), part_at(n)) for n in range(W_PARTS)]
            + [pl.BlockSpec((2, hid, LANES), down_at(other)) for other in range(2)],
            out_specs=[pl.BlockSpec((t // 2, LANES), lambda j, idx: (0, behind(j)))] * 2
            + [pl.BlockSpec((1, 2, k, 2 * LANES), lambda j, idx: (jnp.minimum(j, n_x - 1), 0, 0, 0))],
            scratch_shapes=[
                pltpu.VMEM((feat, 2 * LANES), BF),
                pltpu.VMEM((t + 16, 2 * LANES), F32),
                pltpu.VMEM((t + 16, 2 * LANES), F32),
            ],
        ),
        out_shape=[jax.ShapeDtypeStruct((t // 2, k), BF)] * 2 + [jax.ShapeDtypeStruct((n_x, 2, k, 2 * LANES), BF)],
        compiler_params=pltpu.CompilerParams(vmem_limit_bytes=FEED_MIB * MIB),
        name="feed_in",
    )(idx, normed, big, taps, *([big] * (W_PARTS + 2)))


def give_kernel(h, down, out):
    for turn in range(out.shape[0]):
        out[turn] = jnp.dot(h[...], down[turn, 1], preferred_element_type=F32).astype(BF)


def keep_kernel(h, down, got, here, *sent):
    for turn, out in enumerate((here, *sent)):
        y = jnp.dot(h[...], down[turn, 0], preferred_element_type=F32) + got[turn].astype(F32)
        out[...] = y.astype(out.dtype)


def feed_out(h, down):
    t = h.shape[0]
    n_x, width = down.shape[0], down.shape[3]
    spec = pl.BlockSpec(memory_space=pltpu.VMEM)
    params = pltpu.CompilerParams(vmem_limit_bytes=6 * MIB)
    other = pl.pallas_call(
        give_kernel,
        in_specs=[spec] * 2,
        out_specs=spec,
        out_shape=jax.ShapeDtypeStruct((n_x, t, width), BF),
        compiler_params=params,
        name="give",
    )(h, down)
    return pl.pallas_call(
        keep_kernel,
        in_specs=[spec] * 3,
        out_specs=[spec] * n_x,
        out_shape=[jax.ShapeDtypeStruct((t, width), F32)] + [jax.ShapeDtypeStruct((t, width), BF)] * (n_x - 1),
        compiler_params=params,
        name="keep",
    )(h, down, swap_core(other))


def tiles(gate, up):
    cut = gate.shape[1] // LANES * LANES
    out = []
    for lo in range(0, cut, LANES):
        out += [gate[:, lo : lo + LANES], up[:, lo : lo + LANES]]
    return out + [jnp.concatenate([gate[:, cut:], up[:, cut:]], axis=1)]


def pack_kernel(gate, up, down, gate_taps, up_taps, out, taps):
    parts = tiles(gate[...].T, up[...].T)
    for n, part in enumerate(parts):
        out[n * part.shape[0] : (n + 1) * part.shape[0], :] = part
    out[len(parts) * parts[0].shape[0] :, :] = down[...]
    parts = tiles(gate_taps, up_taps)
    parts.append(jnp.zeros_like(parts[-1]))
    for n in range(taps.shape[0]):
        taps[n] = jnp.concatenate(parts[2 * n : 2 * n + 2], axis=1)


def pack_weights(gate, up, down, gate_taps, up_taps):
    rows = 2 * gate.shape[0] * gate.shape[1] // LANES + down.shape[0]
    pairs = gate.shape[0] // LANES + 1
    spec = pl.BlockSpec(memory_space=pltpu.VMEM)
    return pl.pallas_call(
        pack_kernel,
        in_specs=[spec] * 5,
        out_specs=[spec] * 2,
        out_shape=[
            jax.ShapeDtypeStruct((rows, LANES), BF),
            jax.ShapeDtypeStruct((pairs, gate_taps.shape[0], 2 * LANES), F32),
        ],
        compiler_params=pltpu.CompilerParams(vmem_limit_bytes=6 * MIB),
        name="pack",
    )(*(pltpu.with_memory_space_constraint(a, pltpu.HBM) for a in (gate, up, down, gate_taps, up_taps)))


def sum_tp_small(s):
    s = s + swap_core(s)
    return s + sum(shift(s, "tp", 2 * r) for r in range(1, lax.axis_size("tp") // 2))


def local(
    tokens,
    mix_gain,
    value_proj,
    gate_proj,
    conv_taps,
    chan_gain,
    chan_shift,
    mix_out,
    mlp_gain,
    mlp_gate,
    mlp_up,
    gate_taps,
    up_taps,
    mlp_down,
    final_gain,
):
    n_tp = lax.axis_size("tp")
    n_fs = lax.axis_size("fs")
    idx = jnp.stack([lax.axis_index("tp"), lax.axis_index("fs"), lax.axis_index("grp") % 2]).astype(jnp.int32)
    _, feat = tokens.shape
    hid = mlp_gate.shape[1]
    rows_of = lambda v: v.reshape(n_tp, 1, -1)

    value_gate = jnp.concatenate([value_proj, gate_proj], axis=1)
    quads = quads_fs(jnp.concatenate([half_rows(value_gate), half_rows(mix_out)], axis=0))
    toks = pieces_tp(tokens)

    big, taps = pack_weights(mlp_gate.T, mlp_up.T, mlp_down, gate_taps, up_taps)
    big = pltpu.with_memory_space_constraint(lax.all_gather(big, "fs", axis=0), pltpu.HBM)

    normed = norm_in(idx, toks, rows_of(mix_gain), False)
    conv_out = mixer_in(idx, normed, quads, conv_taps, n_tp, n_fs)
    convs = pieces_tp(conv_out)
    mixed = mixer_out(idx, convs, quads, rows_of(chan_gain), rows_of(chan_shift), tokens, n_fs)
    normed_two = norm_in(idx, pieces_tp(mixed), rows_of(mlp_gain), True)
    *hidden, down = feed_in(idx, normed_two, big, taps, hid, n_tp)

    summed = []
    for n, h in enumerate(hidden):
        rows = h.shape[0]
        here, *sent = feed_out(h, down)
        got = [shift(sent[r - 1], "tp", 2 * r) for r in range(len(sent), 0, -1)]
        total = mixed[n * rows : (n + 1) * rows].astype(F32) + here
        for part in got:
            total = total + part.astype(F32)
        summed.append(total)

    summed = jnp.concatenate(summed, axis=0)
    squares = sum_tp_small(jnp.sum(summed * summed, axis=-1).reshape(-1, LANES)).reshape(-1, 1)
    layer_out = summed * lax.rsqrt(squares / (feat * n_tp) + 1e-06) * final_gain
    return layer_out.astype(BF)


def solution(mesh):
    return jax.shard_map(
        local,
        mesh=mesh,
        in_specs=(
            P(("grp", "fs"), "tp"),
            P(),
            P("fs", "tp"),
            P("fs", "tp"),
            P(None, "tp"),
            P(),
            P(),
            P("fs", "tp"),
            P(),
            P("fs", "tp"),
            P("fs", "tp"),
            P(None, "tp"),
            P(None, "tp"),
            P("tp", "fs"),
            P("tp"),
        ),
        out_specs=P(("grp", "fs"), "tp"),
        check_vma=False,
    )
```

```python
import functools

import jax
import jax.numpy as jnp
from jax import lax
from jax.experimental import pallas as pl
from jax.experimental.pallas import tpu as pltpu
from jax.sharding import PartitionSpec as P


BF = jnp.bfloat16
F32 = jnp.float32
LANES = 128
QUAD_BY = (0, 1, 2, -1)
MIB = 1024 * 1024
FEED_MIB = 20


def shift(a, axis, by):
    n = lax.axis_size(axis)
    return lax.ppermute(a, axis, [(i, (i + by) % n) for i in range(n)])


def swap_core(a):
    n = lax.axis_size("tp")
    return lax.ppermute(a, "tp", [(i, i ^ 1) for i in range(n)])


def swap_group(a):
    n = lax.axis_size("grp")
    return lax.ppermute(a, "grp", [(i, i ^ 1) for i in range(n)])


def half_rows(a):
    rows = a.shape[0] // 2
    return lax.dynamic_slice_in_dim(a, (lax.axis_index("grp") % 2) * rows, rows, 0)


def quads_fs(a):
    q = lax.axis_size("fs") // 4
    quad = jnp.stack([a] + [shift(a, "fs", k * q) for k in (1, 2, 3)])
    quads = [quad] + [shift(quad, "fs", by) for by in QUAD_BY[1:]]
    return quads + [swap_group(piece) for piece in quads]


def pieces_tp(a):
    half = lax.axis_size("tp") // 2
    same = [a] + [shift(a, "tp", 2 * r) for r in range(1, half)]
    out = []
    for piece in same:
        out += [piece, swap_core(piece)]
    return out


def source(pos, me, n):
    return ((me // 2 - pos // 2) % (n // 2)) * 2 + (me % 2 + pos % 2) % 2


def position(src, me, n):
    return ((me // 2 - src // 2) % (n // 2)) * 2 + (me % 2 + src % 2) % 2


def place_quads(idx, quads, buf, lo, rows, n_tp, n_fs):
    per = n_fs // n_tp
    for n, quad in enumerate(quads):
        part = idx[2] if n < 4 else 1 - idx[2]
        for k in range(4):
            f = (idx[1] + 2 * n_fs - QUAD_BY[n % 4] - k * (n_fs // 4)) % n_fs
            at = position(f // per, idx[0] + 2 * n_tp, n_tp) * (2 * per * rows) + (f % per) * 2 * rows + part * rows
            buf[pl.ds(pl.multiple_of(at, rows), rows), :] = quad[k, lo : lo + rows]


def norm_rows(idx, parts, gain, at, store):
    n_tp = len(parts)
    width = parts[0].shape[1]
    total = 0.0
    for part in parts:
        x = part[at, :].astype(F32)
        total = total + x * x
    scale = lax.rsqrt(jnp.sum(total, axis=-1, keepdims=True) / (width * n_tp) + 1e-06)
    for p, part in enumerate(parts):
        src = source(p, idx[0] + 2 * n_tp, n_tp)
        store(p, src, (part[at, :].astype(F32) * scale * gain[src]).astype(BF))


def whole(a):
    return pl.BlockSpec(a.shape, lambda *i: (0,) * a.ndim)


def norm_in_kernel(n_tp, absolute, idx, *refs):
    parts, gain, out = refs[:n_tp], refs[n_tp], refs[n_tp + 1]
    width = parts[0].shape[1]
    chunk = 128

    def store_at(at):
        def store(p, src, value):
            if absolute:
                out[at, pl.ds(pl.multiple_of(src * width, width), width)] = value
            else:
                out[at, p * width : (p + 1) * width] = value

        return store

    for i in range(parts[0].shape[0] // chunk):
        at = slice(i * chunk, (i + 1) * chunk)
        norm_rows(idx, parts, gain, at, store_at(at))


def norm_in(idx, toks, gain, absolute):
    n_tp = len(toks)
    t, width = toks[0].shape
    rows = 256
    return pl.pallas_call(
        functools.partial(norm_in_kernel, n_tp, absolute),
        grid=(t // rows,),
        in_specs=[pl.BlockSpec(memory_space=pltpu.SMEM)]
        + [pl.BlockSpec((rows, width), lambda i: (i, 0))] * n_tp
        + [whole(gain)],
        out_specs=pl.BlockSpec((rows, width * n_tp), lambda i: (i, 0)),
        out_shape=jax.ShapeDtypeStruct((t, width * n_tp), BF),
        compiler_params=pltpu.CompilerParams(vmem_limit_bytes=10 * MIB),
    )(idx, *toks, gain)


def mixer_in_kernel(n_tp, n_fs, idx, normed, *refs):
    quads = refs[:8]
    taps, out, wbuf, gbuf = refs[8:]
    length, chans = out.shape
    pad = 16
    place_quads(idx, quads, wbuf, 0, wbuf.shape[0] // (2 * n_fs), n_tp, n_fs)
    gbuf[0:pad, :] = jnp.zeros((pad, chans), F32)
    gbuf[pad + length :, :] = jnp.zeros((pad, chans), F32)
    both = jnp.dot(normed[...], wbuf[...], preferred_element_type=F32)
    gbuf[pad : pad + length, :] = both[:, :chans] * jax.nn.sigmoid(both[:, chans:])
    n_taps = taps.shape[0]
    first = pad - (n_taps - 1) // 2
    block = 64

    def body(i, carry):
        base = pl.multiple_of(i * block, block)
        acc = jnp.zeros((block, chans), F32)
        for s in range(8):
            win = gbuf[pl.ds(base + first + s, block + 24), :]
            for q in range(4):
                k = s + 8 * q
                if k < n_taps:
                    acc = acc + taps[k : k + 1, :] * win[8 * q : 8 * q + block]
        out[pl.ds(base, block), :] = acc.astype(BF)
        return carry

    lax.fori_loop(0, length // block, body, 0)


def mixer_in(idx, normed, quads, taps, n_tp, n_fs):
    t, feat = normed.shape
    chans = taps.shape[1]
    return pl.pallas_call(
        functools.partial(mixer_in_kernel, n_tp, n_fs),
        grid=(1,),
        in_specs=[pl.BlockSpec(memory_space=pltpu.SMEM), whole(normed)] + [whole(q) for q in quads] + [whole(taps)],
        out_specs=pl.BlockSpec((t, chans), lambda i: (0, 0)),
        out_shape=jax.ShapeDtypeStruct((t, chans), BF),
        scratch_shapes=[
            pltpu.VMEM((feat, 2 * chans), BF),
            pltpu.VMEM((t + 32, chans), F32),
        ],
        compiler_params=pltpu.CompilerParams(vmem_limit_bytes=16 * MIB),
        name="mixer_in",
    )(idx, normed, *quads, taps)


def mixer_out_kernel(n_tp, n_fs, idx, *refs):
    convs, quads = refs[:n_tp], refs[n_tp : n_tp + 8]
    gain, bias, resid, out, wbuf, hbuf = refs[n_tp + 8 :]

    @pl.when(pl.program_id(0) == 0)
    def _():
        rows = wbuf.shape[0] // (2 * n_fs)
        place_quads(idx, quads, wbuf, quads[0].shape[1] - rows, rows, n_tp, n_fs)

    chans = convs[0].shape[1]
    chunk = 128
    for i in range(convs[0].shape[0] // chunk):
        at = slice(i * chunk, (i + 1) * chunk)
        total, square = 0.0, 0.0
        for c in convs:
            x = c[at, :].astype(F32)
            total, square = total + x, square + x * x
        mean = jnp.sum(total, axis=-1, keepdims=True) / (chans * n_tp)
        square = jnp.sum(square, axis=-1, keepdims=True) / (chans * n_tp)
        scale = lax.rsqrt(square - mean * mean + 1e-05)
        for p, c in enumerate(convs):
            src = source(p, idx[0] + 2 * n_tp, n_tp)
            v = (c[at, :].astype(F32) - mean) * scale * gain[src] + bias[src]
            hbuf[at, p * chans : (p + 1) * chans] = (v * jax.nn.sigmoid(v)).astype(BF)
    result = jnp.dot(hbuf[...], wbuf[...], preferred_element_type=F32)
    out[...] = (resid[...].astype(F32) + result).astype(BF)


def mixer_out(idx, convs, quads, gain, bias, resid, n_fs):
    n_tp = len(convs)
    t, chans = convs[0].shape
    width = resid.shape[1]
    rows = 512
    return pl.pallas_call(
        functools.partial(mixer_out_kernel, n_tp, n_fs),
        grid=(t // rows,),
        in_specs=[pl.BlockSpec(memory_space=pltpu.SMEM)]
        + [pl.BlockSpec((rows, chans), lambda i: (i, 0))] * n_tp
        + [whole(q) for q in quads]
        + [whole(gain), whole(bias), pl.BlockSpec((rows, width), lambda i: (i, 0))],
        out_specs=pl.BlockSpec((rows, width), lambda i: (i, 0)),
        out_shape=jax.ShapeDtypeStruct((t, width), BF),
        scratch_shapes=[
            pltpu.VMEM((chans * n_tp, width), BF),
            pltpu.VMEM((rows, chans * n_tp), BF),
        ],
        compiler_params=pltpu.CompilerParams(vmem_limit_bytes=10 * MIB),
        name="mixer_out",
    )(idx, *convs, *quads, gain, bias, resid)


def feed_in_kernel(hid, idx, normed, taps, big, *refs):
    *outs, down_out, w, w_last, down, even, odd, w_sems, down_sems = refs
    t, feat = normed.shape
    full = w.shape[0]
    n_x = down_out.shape[0]
    wide = 2 * LANES
    chunk = 128

    loads = [
        pltpu.make_async_copy(big.at[:, pl.ds(j * wide, wide), :], w.at[j], w_sems.at[j]) for j in range(full)
    ]
    loads.append(pltpu.make_async_copy(big.at[:, pl.ds(full * wide, LANES), :], w_last, w_sems.at[full]))
    down_loads = []
    for turn in range(n_x):
        for other in range(2):
            f = 2 * (2 * ((idx[0] // 2 + turn) % n_x) + (idx[0] % 2 + other) % 2)
            down_loads.append(
                pltpu.make_async_copy(
                    big.at[pl.ds(f, 2), pl.ds(2 * hid, hid), :], down.at[turn, other], down_sems.at[turn, other]
                )
            )
    for load in loads + down_loads:
        load.start()

    for ybuf in (even, odd):
        ybuf[0:8, :] = jnp.zeros((8, wide), F32)
        ybuf[8 + t :, :] = jnp.zeros((8, wide), F32)

    def conv(ybuf, lo, hi, j, lanes):
        tap = taps[j]
        return (
            tap[0:1, lanes] * ybuf[lo + 7 : hi + 7, lanes]
            + tap[1:2, lanes] * ybuf[lo + 8 : hi + 8, lanes]
            + tap[2:3, lanes] * ybuf[lo + 9 : hi + 9, lanes]
        )

    def store(lo, j, value):
        n, at = divmod(lo, outs[0].shape[0])
        outs[n][at : at + chunk, j * LANES : (j + 1) * LANES] = value.astype(BF)

    for j in range(full + 2):
        now, before = (even, odd) if j % 2 == 0 else (odd, even)
        if j < full:
            loads[j].wait()
            both = jnp.concatenate(
                [w[j, :, :LANES].reshape(feat, LANES), w[j, :, LANES:].reshape(feat, LANES)], axis=1
            )
            now[8 : 8 + t, :] = jnp.dot(normed[...], both, preferred_element_type=F32)
        elif j == full:
            loads[j].wait()
            now[8 : 8 + t, :LANES] = jnp.dot(
                normed[...], w_last[...].reshape(feat, LANES), preferred_element_type=F32
            )
        if 0 < j <= full:
            for lo in range(0, t, chunk):
                g = conv(before, lo, lo + chunk, j - 1, slice(0, LANES))
                u = conv(before, lo, lo + chunk, j - 1, slice(LANES, wide))
                store(lo, j - 1, g * jax.nn.sigmoid(g) * u)
        if j == full + 1:
            for lo in range(0, t, chunk):
                g = conv(before, lo, lo + chunk, full, slice(0, LANES))
                h = g * jax.nn.sigmoid(g) * pltpu.roll(g, LANES // 2, 1)
                lane = lax.broadcasted_iota(jnp.int32, h.shape, 1)
                store(lo, full, jnp.where(lane < LANES // 2, h, 0.0))

    for load in down_loads:
        load.wait()
    for turn in range(n_x):
        for other in range(2):
            down_out[turn, other, :hid, :LANES] = down[turn, other, 0]
            down_out[turn, other, :hid, LANES:] = down[turn, other, 1]
            down_out[turn, other, hid:, :] = jnp.zeros((down_out.shape[2] - hid, wide), BF)


def feed_in(idx, normed, big, taps, hid, n_tp):
    t, _ = normed.shape
    full = hid // LANES
    n_fs = big.shape[0]
    n_x = n_tp // 2
    k = (full + 1) * LANES
    spec = pl.BlockSpec(memory_space=pltpu.VMEM)
    return pl.pallas_call(
        functools.partial(feed_in_kernel, hid),
        in_specs=[pl.BlockSpec(memory_space=pltpu.SMEM), spec, spec, pl.BlockSpec(memory_space=pltpu.HBM)],
        out_specs=[spec] * 3,
        out_shape=[jax.ShapeDtypeStruct((t // 2, k), BF)] * 2 + [jax.ShapeDtypeStruct((n_x, 2, k, 2 * LANES), BF)],
        scratch_shapes=[
            pltpu.VMEM((full, n_fs, 2 * LANES, LANES), BF),
            pltpu.VMEM((n_fs, LANES, LANES), BF),
            pltpu.VMEM((n_x, 2, 2, hid, LANES), BF),
            pltpu.VMEM((t + 16, 2 * LANES), F32),
            pltpu.VMEM((t + 16, 2 * LANES), F32),
            pltpu.SemaphoreType.DMA((full + 1,)),
            pltpu.SemaphoreType.DMA((n_x, 2)),
        ],
        compiler_params=pltpu.CompilerParams(vmem_limit_bytes=FEED_MIB * MIB),
        name="feed_in",
    )(idx, normed, taps, big)


def give_kernel(h, down, out):
    for turn in range(out.shape[0]):
        out[turn] = jnp.dot(h[...], down[turn, 1], preferred_element_type=F32).astype(BF)


def keep_kernel(h, down, got, here, *sent):
    for turn, out in enumerate((here, *sent)):
        y = jnp.dot(h[...], down[turn, 0], preferred_element_type=F32) + got[turn].astype(F32)
        out[...] = y.astype(out.dtype)


def feed_out(h, down):
    t = h.shape[0]
    n_x, width = down.shape[0], down.shape[3]
    spec = pl.BlockSpec(memory_space=pltpu.VMEM)
    params = pltpu.CompilerParams(vmem_limit_bytes=6 * MIB)
    other = pl.pallas_call(
        give_kernel,
        in_specs=[spec] * 2,
        out_specs=spec,
        out_shape=jax.ShapeDtypeStruct((n_x, t, width), BF),
        compiler_params=params,
        name="give",
    )(h, down)
    return pl.pallas_call(
        keep_kernel,
        in_specs=[spec] * 3,
        out_specs=[spec] * n_x,
        out_shape=[jax.ShapeDtypeStruct((t, width), F32)] + [jax.ShapeDtypeStruct((t, width), BF)] * (n_x - 1),
        compiler_params=params,
        name="keep",
    )(h, down, swap_core(other))


def tiles(gate, up):
    cut = gate.shape[1] // LANES * LANES
    out = []
    for lo in range(0, cut, LANES):
        out += [gate[:, lo : lo + LANES], up[:, lo : lo + LANES]]
    return out + [jnp.concatenate([gate[:, cut:], up[:, cut:]], axis=1)]


def pack_kernel(gate, up, down, gate_taps, up_taps, out, taps):
    parts = tiles(gate[...].T, up[...].T)
    for n, part in enumerate(parts):
        out[n * part.shape[0] : (n + 1) * part.shape[0], :] = part
    out[len(parts) * parts[0].shape[0] :, :] = down[...]
    parts = tiles(gate_taps, up_taps)
    parts.append(jnp.zeros_like(parts[-1]))
    for n in range(taps.shape[0]):
        taps[n] = jnp.concatenate(parts[2 * n : 2 * n + 2], axis=1)


def pack_weights(gate, up, down, gate_taps, up_taps):
    rows = 2 * gate.shape[0] * gate.shape[1] // LANES + down.shape[0]
    pairs = gate.shape[0] // LANES + 1
    spec = pl.BlockSpec(memory_space=pltpu.VMEM)
    return pl.pallas_call(
        pack_kernel,
        in_specs=[spec] * 5,
        out_specs=[spec] * 2,
        out_shape=[
            jax.ShapeDtypeStruct((rows, LANES), BF),
            jax.ShapeDtypeStruct((pairs, gate_taps.shape[0], 2 * LANES), F32),
        ],
        compiler_params=pltpu.CompilerParams(vmem_limit_bytes=6 * MIB),
        name="pack",
    )(*(pltpu.with_memory_space_constraint(a, pltpu.HBM) for a in (gate, up, down, gate_taps, up_taps)))


def sum_tp_small(s):
    s = s + swap_core(s)
    return s + sum(shift(s, "tp", 2 * r) for r in range(1, lax.axis_size("tp") // 2))


def local(
    tokens,
    mix_gain,
    value_proj,
    gate_proj,
    conv_taps,
    chan_gain,
    chan_shift,
    mix_out,
    mlp_gain,
    mlp_gate,
    mlp_up,
    gate_taps,
    up_taps,
    mlp_down,
    final_gain,
):
    n_tp = lax.axis_size("tp")
    n_fs = lax.axis_size("fs")
    idx = jnp.stack([lax.axis_index("tp"), lax.axis_index("fs"), lax.axis_index("grp") % 2]).astype(jnp.int32)
    _, feat = tokens.shape
    hid = mlp_gate.shape[1]
    rows_of = lambda v: v.reshape(n_tp, 1, -1)

    value_gate = jnp.concatenate([value_proj, gate_proj], axis=1)
    quads = quads_fs(jnp.concatenate([half_rows(value_gate), half_rows(mix_out)], axis=0))
    toks = pieces_tp(tokens)

    big, taps = pack_weights(mlp_gate.T, mlp_up.T, mlp_down, gate_taps, up_taps)
    big = pltpu.with_memory_space_constraint(lax.all_gather(big, "fs", axis=0), pltpu.HBM)

    normed = norm_in(idx, toks, rows_of(mix_gain), False)
    conv_out = mixer_in(idx, normed, quads, conv_taps, n_tp, n_fs)
    convs = pieces_tp(conv_out)
    mixed = mixer_out(idx, convs, quads, rows_of(chan_gain), rows_of(chan_shift), tokens, n_fs)
    normed_two = norm_in(idx, pieces_tp(mixed), rows_of(mlp_gain), True)
    *hidden, down = feed_in(idx, normed_two, big, taps, hid, n_tp)

    summed = []
    for n, h in enumerate(hidden):
        rows = h.shape[0]
        here, *sent = feed_out(h, down)
        got = [shift(sent[r - 1], "tp", 2 * r) for r in range(len(sent), 0, -1)]
        total = mixed[n * rows : (n + 1) * rows].astype(F32) + here
        for part in got:
            total = total + part.astype(F32)
        summed.append(total)

    summed = jnp.concatenate(summed, axis=0)
    squares = sum_tp_small(jnp.sum(summed * summed, axis=-1).reshape(-1, LANES)).reshape(-1, 1)
    layer_out = summed * lax.rsqrt(squares / (feat * n_tp) + 1e-06) * final_gain
    return layer_out.astype(BF)


def solution(mesh):
    return jax.shard_map(
        local,
        mesh=mesh,
        in_specs=(
            P(("grp", "fs"), "tp"),
            P(),
            P("fs", "tp"),
            P("fs", "tp"),
            P(None, "tp"),
            P(),
            P(),
            P("fs", "tp"),
            P(),
            P("fs", "tp"),
            P("fs", "tp"),
            P(None, "tp"),
            P(None, "tp"),
            P("tp", "fs"),
            P("tp"),
        ),
        out_specs=P(("grp", "fs"), "tp"),
        check_vma=False,
    )
```

```python
import functools

import jax
import jax.numpy as jnp
from jax import lax
from jax.experimental import pallas as pl
from jax.experimental.pallas import tpu as pltpu
from jax.sharding import PartitionSpec as P


BF = jnp.bfloat16
F32 = jnp.float32
LANES = 128
QUAD_BY = (0, 1, 2, -1)
MIB = 1024 * 1024
FEED_MIB = 16


def shift(a, axis, by):
    n = lax.axis_size(axis)
    return lax.ppermute(a, axis, [(i, (i + by) % n) for i in range(n)])


def swap_core(a):
    n = lax.axis_size("tp")
    return lax.ppermute(a, "tp", [(i, i ^ 1) for i in range(n)])


def swap_group(a):
    n = lax.axis_size("grp")
    return lax.ppermute(a, "grp", [(i, i ^ 1) for i in range(n)])


def half_rows(a):
    rows = a.shape[0] // 2
    return lax.dynamic_slice_in_dim(a, (lax.axis_index("grp") % 2) * rows, rows, 0)


def quads_fs(a):
    q = lax.axis_size("fs") // 4
    quad = jnp.stack([a] + [shift(a, "fs", k * q) for k in (1, 2, 3)])
    quads = [quad] + [shift(quad, "fs", by) for by in QUAD_BY[1:]]
    return quads + [swap_group(piece) for piece in quads]


def pieces_tp(a):
    half = lax.axis_size("tp") // 2
    same = [a] + [shift(a, "tp", 2 * r) for r in range(1, half)]
    out = []
    for piece in same:
        out += [piece, swap_core(piece)]
    return out


def source(pos, me, n):
    return ((me // 2 - pos // 2) % (n // 2)) * 2 + (me % 2 + pos % 2) % 2


def position(src, me, n):
    return ((me // 2 - src // 2) % (n // 2)) * 2 + (me % 2 + src % 2) % 2


def place_quads(idx, quads, buf, lo, rows, n_tp, n_fs):
    per = n_fs // n_tp
    for n, quad in enumerate(quads):
        part = idx[2] if n < 4 else 1 - idx[2]
        for k in range(4):
            f = (idx[1] + 2 * n_fs - QUAD_BY[n % 4] - k * (n_fs // 4)) % n_fs
            at = position(f // per, idx[0] + 2 * n_tp, n_tp) * (2 * per * rows) + (f % per) * 2 * rows + part * rows
            buf[pl.ds(pl.multiple_of(at, rows), rows), :] = quad[k, lo : lo + rows]


def norm_rows(idx, parts, gain, at, store):
    n_tp = len(parts)
    width = parts[0].shape[1]
    total = 0.0
    for part in parts:
        x = part[at, :].astype(F32)
        total = total + x * x
    scale = lax.rsqrt(jnp.sum(total, axis=-1, keepdims=True) / (width * n_tp) + 1e-06)
    for p, part in enumerate(parts):
        src = source(p, idx[0] + 2 * n_tp, n_tp)
        store(p, src, (part[at, :].astype(F32) * scale * gain[src]).astype(BF))


def whole(a):
    return pl.BlockSpec(a.shape, lambda *i: (0,) * a.ndim)


def norm_in_kernel(n_tp, absolute, idx, *refs):
    parts, gain, out = refs[:n_tp], refs[n_tp], refs[n_tp + 1]
    width = parts[0].shape[1]
    chunk = 128

    def store_at(at):
        def store(p, src, value):
            if absolute:
                out[at, pl.ds(pl.multiple_of(src * width, width), width)] = value
            else:
                out[at, p * width : (p + 1) * width] = value

        return store

    for i in range(parts[0].shape[0] // chunk):
        at = slice(i * chunk, (i + 1) * chunk)
        norm_rows(idx, parts, gain, at, store_at(at))


def norm_in(idx, toks, gain, absolute):
    n_tp = len(toks)
    t, width = toks[0].shape
    rows = 256
    return pl.pallas_call(
        functools.partial(norm_in_kernel, n_tp, absolute),
        grid=(t // rows,),
        in_specs=[pl.BlockSpec(memory_space=pltpu.SMEM)]
        + [pl.BlockSpec((rows, width), lambda i: (i, 0))] * n_tp
        + [whole(gain)],
        out_specs=pl.BlockSpec((rows, width * n_tp), lambda i: (i, 0)),
        out_shape=jax.ShapeDtypeStruct((t, width * n_tp), BF),
        compiler_params=pltpu.CompilerParams(vmem_limit_bytes=10 * MIB),
    )(idx, *toks, gain)


def mixer_in_kernel(n_tp, n_fs, idx, normed, *refs):
    quads = refs[:8]
    taps, out, wbuf, gbuf = refs[8:]
    length, chans = out.shape
    pad = 16
    place_quads(idx, quads, wbuf, 0, wbuf.shape[0] // (2 * n_fs), n_tp, n_fs)
    gbuf[0:pad, :] = jnp.zeros((pad, chans), F32)
    gbuf[pad + length :, :] = jnp.zeros((pad, chans), F32)
    both = jnp.dot(normed[...], wbuf[...], preferred_element_type=F32)
    gbuf[pad : pad + length, :] = both[:, :chans] * jax.nn.sigmoid(both[:, chans:])
    n_taps = taps.shape[0]
    first = pad - (n_taps - 1) // 2
    block = 64

    def body(i, carry):
        base = pl.multiple_of(i * block, block)
        acc = jnp.zeros((block, chans), F32)
        for s in range(8):
            win = gbuf[pl.ds(base + first + s, block + 24), :]
            for q in range(4):
                k = s + 8 * q
                if k < n_taps:
                    acc = acc + taps[k : k + 1, :] * win[8 * q : 8 * q + block]
        out[pl.ds(base, block), :] = acc.astype(BF)
        return carry

    lax.fori_loop(0, length // block, body, 0)


def mixer_in(idx, normed, quads, taps, n_tp, n_fs):
    t, feat = normed.shape
    chans = taps.shape[1]
    return pl.pallas_call(
        functools.partial(mixer_in_kernel, n_tp, n_fs),
        grid=(1,),
        in_specs=[pl.BlockSpec(memory_space=pltpu.SMEM), whole(normed)] + [whole(q) for q in quads] + [whole(taps)],
        out_specs=pl.BlockSpec((t, chans), lambda i: (0, 0)),
        out_shape=jax.ShapeDtypeStruct((t, chans), BF),
        scratch_shapes=[
            pltpu.VMEM((feat, 2 * chans), BF),
            pltpu.VMEM((t + 32, chans), F32),
        ],
        compiler_params=pltpu.CompilerParams(vmem_limit_bytes=16 * MIB),
        name="mixer_in",
    )(idx, normed, *quads, taps)


def mixer_out_kernel(n_tp, n_fs, idx, *refs):
    convs, quads = refs[:n_tp], refs[n_tp : n_tp + 8]
    gain, bias, resid, out, wbuf, hbuf = refs[n_tp + 8 :]

    @pl.when(pl.program_id(0) == 0)
    def _():
        rows = wbuf.shape[0] // (2 * n_fs)
        place_quads(idx, quads, wbuf, quads[0].shape[1] - rows, rows, n_tp, n_fs)

    chans = convs[0].shape[1]
    chunk = 128
    for i in range(convs[0].shape[0] // chunk):
        at = slice(i * chunk, (i + 1) * chunk)
        total, square = 0.0, 0.0
        for c in convs:
            x = c[at, :].astype(F32)
            total, square = total + x, square + x * x
        mean = jnp.sum(total, axis=-1, keepdims=True) / (chans * n_tp)
        square = jnp.sum(square, axis=-1, keepdims=True) / (chans * n_tp)
        scale = lax.rsqrt(square - mean * mean + 1e-05)
        for p, c in enumerate(convs):
            src = source(p, idx[0] + 2 * n_tp, n_tp)
            v = (c[at, :].astype(F32) - mean) * scale * gain[src] + bias[src]
            hbuf[at, p * chans : (p + 1) * chans] = (v * jax.nn.sigmoid(v)).astype(BF)
    result = jnp.dot(hbuf[...], wbuf[...], preferred_element_type=F32)
    out[...] = (resid[...].astype(F32) + result).astype(BF)


def mixer_out(idx, convs, quads, gain, bias, resid, n_fs):
    n_tp = len(convs)
    t, chans = convs[0].shape
    width = resid.shape[1]
    rows = 512
    return pl.pallas_call(
        functools.partial(mixer_out_kernel, n_tp, n_fs),
        grid=(t // rows,),
        in_specs=[pl.BlockSpec(memory_space=pltpu.SMEM)]
        + [pl.BlockSpec((rows, chans), lambda i: (i, 0))] * n_tp
        + [whole(q) for q in quads]
        + [whole(gain), whole(bias), pl.BlockSpec((rows, width), lambda i: (i, 0))],
        out_specs=pl.BlockSpec((rows, width), lambda i: (i, 0)),
        out_shape=jax.ShapeDtypeStruct((t, width), BF),
        scratch_shapes=[
            pltpu.VMEM((chans * n_tp, width), BF),
            pltpu.VMEM((rows, chans * n_tp), BF),
        ],
        compiler_params=pltpu.CompilerParams(vmem_limit_bytes=10 * MIB),
        name="mixer_out",
    )(idx, *convs, *quads, gain, bias, resid)


def feed_in_kernel(n_x, idx, normed, w_last, taps, w, *refs):
    down = refs[:2]
    *outs, down_out, even, odd = refs[2:]
    step = pl.program_id(0)
    last = pl.num_programs(0) - 1
    t, feat = normed.shape
    chunk = 128

    @pl.when(step < n_x)
    def _():
        hid = down[0].shape[1]
        for core in range(2):
            down_out[0, core, :hid, :LANES] = down[core][0]
            down_out[0, core, :hid, LANES:] = down[core][1]
            down_out[0, core, hid:, :] = jnp.zeros((down_out.shape[2] - hid, 2 * LANES), BF)

    @pl.when(step == 0)
    def _():
        for ybuf in (even, odd):
            ybuf[0:8, :] = jnp.zeros((8, 2 * LANES), F32)
            ybuf[8 + t :, :] = jnp.zeros((8, 2 * LANES), F32)

    def conv(ybuf, lo, hi, lanes):
        tap = taps[0]
        return (
            tap[0:1, lanes] * ybuf[lo + 7 : hi + 7, lanes]
            + tap[1:2, lanes] * ybuf[lo + 8 : hi + 8, lanes]
            + tap[2:3, lanes] * ybuf[lo + 9 : hi + 9, lanes]
        )

    def store(lo, value):
        n, at = divmod(lo, outs[0].shape[0])
        outs[n][at : at + chunk, :] = value.astype(BF)

    def activate(ybuf):
        for lo in range(0, t, chunk):
            g = conv(ybuf, lo, lo + chunk, slice(0, LANES))
            u = conv(ybuf, lo, lo + chunk, slice(LANES, 2 * LANES))
            store(lo, g * jax.nn.sigmoid(g) * u)

    for parity, now, before in ((0, even, odd), (1, odd, even)):

        @pl.when((step % 2 == parity) & (step < last - 1))
        def _():
            block = w[...]
            both = jnp.concatenate(
                [block[:, :LANES].reshape(feat, LANES), block[:, LANES:].reshape(feat, LANES)], axis=1
            )
            activate(before)
            now[8 : 8 + t, :] = jnp.dot(normed[...], both, preferred_element_type=F32)

        @pl.when((step % 2 == parity) & (step == last - 1))
        def _():
            activate(before)
            now[8 : 8 + t, :LANES] = jnp.dot(
                normed[...], w_last[...].reshape(feat, LANES), preferred_element_type=F32
            )

        @pl.when((step % 2 == parity) & (step == last))
        def _():
            for lo in range(0, t, chunk):
                g = conv(before, lo, lo + chunk, slice(0, LANES))
                h = g * jax.nn.sigmoid(g) * pltpu.roll(g, LANES // 2, 1)
                lane = lax.broadcasted_iota(jnp.int32, h.shape, 1)
                store(lo, jnp.where(lane < LANES // 2, h, 0.0))


def feed_in(idx, normed, big, taps, hid, n_tp):
    t, _ = normed.shape
    full = hid // LANES
    n_fs, total, _ = big.shape
    n_x = n_tp // 2
    k = (full + 1) * LANES
    fixed = lambda a: pl.BlockSpec(a.shape, lambda j, idx: (0,) * a.ndim)
    behind = lambda j: jnp.maximum(j - 1, 0)

    def down_at(other):
        def index(j, idx):
            x = (idx[0] // 2 + jnp.minimum(j, n_x - 1)) % n_x
            return (2 * x + (idx[0] % 2 + other) % 2, total // hid - 1, 0)

        return index

    return pl.pallas_call(
        functools.partial(feed_in_kernel, n_x),
        grid_spec=pltpu.PrefetchScalarGridSpec(
            num_scalar_prefetch=1,
            grid=(full + 2,),
            in_specs=[
                fixed(normed),
                pl.BlockSpec((n_fs, LANES, LANES), lambda j, idx: (0, 2 * full, 0)),
                pl.BlockSpec((1,) + taps.shape[1:], lambda j, idx: (behind(j), 0, 0)),
            ]
            + [pl.BlockSpec((n_fs, 2 * LANES, LANES), lambda j, idx: (0, jnp.minimum(j, full - 1), 0))]
            + [pl.BlockSpec((2, hid, LANES), down_at(other)) for other in range(2)],
            out_specs=[pl.BlockSpec((t // 2, LANES), lambda j, idx: (0, behind(j)))] * 2
            + [pl.BlockSpec((1, 2, k, 2 * LANES), lambda j, idx: (jnp.minimum(j, n_x - 1), 0, 0, 0))],
            scratch_shapes=[
                pltpu.VMEM((t + 16, 2 * LANES), F32),
                pltpu.VMEM((t + 16, 2 * LANES), F32),
            ],
        ),
        out_shape=[jax.ShapeDtypeStruct((t // 2, k), BF)] * 2 + [jax.ShapeDtypeStruct((n_x, 2, k, 2 * LANES), BF)],
        compiler_params=pltpu.CompilerParams(vmem_limit_bytes=FEED_MIB * MIB),
        name="feed_in",
    )(idx, normed, big, taps, big, big, big)


def give_kernel(h, down, out):
    for turn in range(out.shape[0]):
        out[turn] = jnp.dot(h[...], down[turn, 1], preferred_element_type=F32).astype(BF)


def keep_kernel(h, down, got, here, *sent):
    for turn, out in enumerate((here, *sent)):
        y = jnp.dot(h[...], down[turn, 0], preferred_element_type=F32) + got[turn].astype(F32)
        out[...] = y.astype(out.dtype)


def feed_out(h, down):
    t = h.shape[0]
    n_x, width = down.shape[0], down.shape[3]
    spec = pl.BlockSpec(memory_space=pltpu.VMEM)
    params = pltpu.CompilerParams(vmem_limit_bytes=6 * MIB)
    other = pl.pallas_call(
        give_kernel,
        in_specs=[spec] * 2,
        out_specs=spec,
        out_shape=jax.ShapeDtypeStruct((n_x, t, width), BF),
        compiler_params=params,
        name="give",
    )(h, down)
    return pl.pallas_call(
        keep_kernel,
        in_specs=[spec] * 3,
        out_specs=[spec] * n_x,
        out_shape=[jax.ShapeDtypeStruct((t, width), F32)] + [jax.ShapeDtypeStruct((t, width), BF)] * (n_x - 1),
        compiler_params=params,
        name="keep",
    )(h, down, swap_core(other))


def tiles(gate, up):
    cut = gate.shape[1] // LANES * LANES
    out = []
    for lo in range(0, cut, LANES):
        out += [gate[:, lo : lo + LANES], up[:, lo : lo + LANES]]
    return out + [jnp.concatenate([gate[:, cut:], up[:, cut:]], axis=1)]


def pack_kernel(gate, up, down, gate_taps, up_taps, out, taps):
    parts = tiles(gate[...].T, up[...].T)
    for n, part in enumerate(parts):
        out[n * part.shape[0] : (n + 1) * part.shape[0], :] = part
    out[len(parts) * parts[0].shape[0] :, :] = down[...]
    parts = tiles(gate_taps, up_taps)
    parts.append(jnp.zeros_like(parts[-1]))
    for n in range(taps.shape[0]):
        taps[n] = jnp.concatenate(parts[2 * n : 2 * n + 2], axis=1)


def pack_weights(gate, up, down, gate_taps, up_taps):
    rows = 2 * gate.shape[0] * gate.shape[1] // LANES + down.shape[0]
    pairs = gate.shape[0] // LANES + 1
    spec = pl.BlockSpec(memory_space=pltpu.VMEM)
    return pl.pallas_call(
        pack_kernel,
        in_specs=[spec] * 5,
        out_specs=[spec] * 2,
        out_shape=[
            jax.ShapeDtypeStruct((rows, LANES), BF),
            jax.ShapeDtypeStruct((pairs, gate_taps.shape[0], 2 * LANES), F32),
        ],
        compiler_params=pltpu.CompilerParams(vmem_limit_bytes=6 * MIB),
        name="pack",
    )(*(pltpu.with_memory_space_constraint(a, pltpu.HBM) for a in (gate, up, down, gate_taps, up_taps)))


def sum_tp_small(s):
    s = s + swap_core(s)
    return s + sum(shift(s, "tp", 2 * r) for r in range(1, lax.axis_size("tp") // 2))


def local(
    tokens,
    mix_gain,
    value_proj,
    gate_proj,
    conv_taps,
    chan_gain,
    chan_shift,
    mix_out,
    mlp_gain,
    mlp_gate,
    mlp_up,
    gate_taps,
    up_taps,
    mlp_down,
    final_gain,
):
    n_tp = lax.axis_size("tp")
    n_fs = lax.axis_size("fs")
    idx = jnp.stack([lax.axis_index("tp"), lax.axis_index("fs"), lax.axis_index("grp") % 2]).astype(jnp.int32)
    _, feat = tokens.shape
    hid = mlp_gate.shape[1]
    rows_of = lambda v: v.reshape(n_tp, 1, -1)

    value_gate = jnp.concatenate([value_proj, gate_proj], axis=1)
    quads = quads_fs(jnp.concatenate([half_rows(value_gate), half_rows(mix_out)], axis=0))
    toks = pieces_tp(tokens)

    big, taps = pack_weights(mlp_gate.T, mlp_up.T, mlp_down, gate_taps, up_taps)
    big = pltpu.with_memory_space_constraint(lax.all_gather(big, "fs", axis=0), pltpu.HBM)

    normed = norm_in(idx, toks, rows_of(mix_gain), False)
    conv_out = mixer_in(idx, normed, quads, conv_taps, n_tp, n_fs)
    convs = pieces_tp(conv_out)
    mixed = mixer_out(idx, convs, quads, rows_of(chan_gain), rows_of(chan_shift), tokens, n_fs)
    normed_two = norm_in(idx, pieces_tp(mixed), rows_of(mlp_gain), True)
    *hidden, down = feed_in(idx, normed_two, big, taps, hid, n_tp)

    summed = []
    for n, h in enumerate(hidden):
        rows = h.shape[0]
        here, *sent = feed_out(h, down)
        got = [shift(sent[r - 1], "tp", 2 * r) for r in range(len(sent), 0, -1)]
        total = mixed[n * rows : (n + 1) * rows].astype(F32) + here
        for part in got:
            total = total + part.astype(F32)
        summed.append(total)

    summed = jnp.concatenate(summed, axis=0)
    squares = sum_tp_small(jnp.sum(summed * summed, axis=-1).reshape(-1, LANES)).reshape(-1, 1)
    layer_out = summed * lax.rsqrt(squares / (feat * n_tp) + 1e-06) * final_gain
    return layer_out.astype(BF)


def solution(mesh):
    return jax.shard_map(
        local,
        mesh=mesh,
        in_specs=(
            P(("grp", "fs"), "tp"),
            P(),
            P("fs", "tp"),
            P("fs", "tp"),
            P(None, "tp"),
            P(),
            P(),
            P("fs", "tp"),
            P(),
            P("fs", "tp"),
            P("fs", "tp"),
            P(None, "tp"),
            P(None, "tp"),
            P("tp", "fs"),
            P("tp"),
        ),
        out_specs=P(("grp", "fs"), "tp"),
        check_vma=False,
    )
```
